512 devices in a mesh: sp: 16 (over z), tp: 32 (over y, x, core).
Axes of the slice: x: 4, y: 4, z: 16, core: 2. Of those that a mesh axis runs over, the one named last changes fastest.
Arguments:
- target: bfloat16 [2048, 2048], P('sp'), may hold values from -6 to 6
- source: bfloat16 [4096, 2048], P(('sp', 'tp')), may hold values from -6 to 6
- cotangent: bfloat16 [2048, 2048], P('sp'), may hold values from -6 to 6
- target_gain: float32 [2048], replicated, may hold values from 0.1 to 1.9
- source_gain: float32 [2048], replicated, may hold values from 0.1 to 1.9
- query_weight: bfloat16 [2048, 8192], P(None, 'tp'), may hold values from -4 to 4
- key_weight: bfloat16 [2048, 2048], P(None, 'tp'), may hold values from -1 to 1
- value_projection_weight: bfloat16 [2048, 2048], P(None, 'tp'), may hold values from -0.125 to 0.125
- output_weight: bfloat16 [8192, 2048], P('tp'), may hold values from -0.0625 to 0.0625
Outputs:
- target_grad: float32 [2048, 2048], P(('sp', 'tp'))
- source_grad: float32 [4096, 2048], P(('sp', 'tp'))
- key_weight_grad: float32 [2048, 2048], P(None, 'tp')
The draws below stay inside these ranges and needn't reach their ends.
All inputs are finite; a program needn't handle non-finite values.
Results may differ from the reference program's by a relative error of at most 0.018.
The reference program's roundings to bfloat16 on the way count: a program that leaves them out, or rounds other values in their place, can miss the bound.
Values may be sent and summed in bfloat16 or wider, within the bound.
A program may use at most 64 MiB of HBM per device.

```python
import jax
import jax.numpy as jnp
from jax import lax

MODEL_WIDTH = 2048
QUERY_HEADS = 32
KEY_VALUE_HEADS = 8
HEAD_SIZE = 256
TGT = 2048
SOURCE_TOTAL = 4096


def drawn_rows(key):
    folded = jax.random.fold_in(key, 11)
    target_key, source_key = jax.random.split(folded, 2)
    source_rows = jax.random.normal(source_key, (SOURCE_TOTAL, MODEL_WIDTH), jnp.float32)
    target_rows = jax.random.normal(target_key, (TGT, MODEL_WIDTH), jnp.float32)
    return (jnp.clip(target_rows, -6.0, 6.0), jnp.clip(source_rows, -6.0, 6.0))


def paired_weights(key):
    folded = jax.random.fold_in(key, 23)
    key_portion, query_part = jax.random.split(folded, 2)
    key_projection_matrix = jnp.clip(jax.random.normal(key_portion, (MODEL_WIDTH, KEY_VALUE_HEADS * HEAD_SIZE), jnp.float32) * MODEL_WIDTH ** (-0.5), -1.0, 1.0)
    query_matrix = jax.random.normal(query_part, (MODEL_WIDTH, QUERY_HEADS * HEAD_SIZE), jnp.float32) * MODEL_WIDTH ** (-0.5)
    return (jnp.clip(query_matrix, -4.0, 4.0), key_projection_matrix)


def draw_target(key, part):
    return drawn_rows(key)[0].astype(jnp.bfloat16)


def draw_source(key, part):
    return drawn_rows(key)[1].astype(jnp.bfloat16)


def draw_query_weight(key, part):
    return paired_weights(key)[0].astype(jnp.bfloat16)


def draw_key_weight(key, part):
    return paired_weights(key)[1].astype(jnp.bfloat16)


def level_of(stream_key, shape, pieces, smallest, largest):
    level = 1.0
    for position, parts in pieces:
        steps = jax.random.uniform(jax.random.fold_in(jax.random.fold_in(stream_key, 6), position), (parts,), jnp.float32, smallest / len(pieces), largest / len(pieces))
        level = level * jnp.repeat(jnp.exp(steps), shape[position] // parts).reshape((-1,) + (1,) * (len(shape) - 1 - position))
    return level


def gaussian(key, extent, deviation, bound, pieces=(), kind=jnp.bfloat16):
    drawn = deviation * jax.random.normal(key, extent, jnp.float32)
    if pieces:
        drawn = drawn * level_of(key, extent, pieces, -0.22, 0.18)
    return jnp.clip(drawn, -bound, bound).astype(kind)


def setup_inputs(seed: int = 0) -> dict:
    key_list = jax.random.split(jax.random.key(seed), 10)
    target = draw_target(jax.random.fold_in(key_list[9], 71), 0)
    source = draw_source(jax.random.fold_in(key_list[9], 71), 0)
    cotangent = gaussian(key_list[2], (TGT, MODEL_WIDTH), 1.0, 6.0, ((0, 16),))
    target_gain = jnp.clip(1.0 + 0.18 * jax.random.normal(key_list[3], (MODEL_WIDTH,), jnp.float32), 0.1, 1.9)
    source_gain = jnp.clip(1.0 + 0.18 * jax.random.normal(key_list[4], (MODEL_WIDTH,), jnp.float32), 0.1, 1.9)
    query_weight = draw_query_weight(jax.random.fold_in(key_list[9], 71), 0)
    key_weight = draw_key_weight(jax.random.fold_in(key_list[9], 71), 0)
    value_projection_weight = gaussian(key_list[7], (MODEL_WIDTH, KEY_VALUE_HEADS * HEAD_SIZE), MODEL_WIDTH ** -0.5, 0.125, ((1, 32),))
    output_weight = gaussian(key_list[8], (QUERY_HEADS * HEAD_SIZE, MODEL_WIDTH), (QUERY_HEADS * HEAD_SIZE) ** -0.5, 0.0625, ((0, 32),))
    return {"target": target, "source": source, "cotangent": cotangent, "target_gain": target_gain, "source_gain": source_gain, "query_weight": query_weight, "key_weight": key_weight, "value_projection_weight": value_projection_weight, "output_weight": output_weight}


EPSILON = 1e-05

def norm_rows(rows):
    values = rows.astype(jnp.float32)
    centred = values - lax.optimization_barrier(jnp.mean(values, axis=-1, keepdims=True))
    inverse = lax.rsqrt(lax.optimization_barrier(jnp.mean(centred * centred, axis=-1, keepdims=True)) + EPSILON)
    return (centred * inverse, inverse)

def norm_back(scaled, inverse, gain, upstream):
    weighted = upstream * gain
    spread = lax.optimization_barrier(jnp.mean(weighted * scaled, axis=-1, keepdims=True))
    return inverse * (weighted - lax.optimization_barrier(jnp.mean(weighted, axis=-1, keepdims=True)) - scaled * spread)

def reference(target, source, cotangent, target_gain, source_gain, query_weight, key_weight, value_projection_weight, output_weight):
    tgt_scaled, tgt_inverse = norm_rows(target)
    tgt_normed = (tgt_scaled * target_gain).astype(jnp.bfloat16)
    src_scaled, src_inverse = norm_rows(source)
    src_normed = (src_scaled * source_gain).astype(jnp.bfloat16)
    queries = jnp.dot(tgt_normed, query_weight, preferred_element_type=jnp.float32).astype(jnp.bfloat16)
    key_rows = jnp.dot(src_normed, key_weight, preferred_element_type=jnp.float32).astype(jnp.bfloat16)
    value_rows = jnp.dot(src_normed, value_projection_weight, preferred_element_type=jnp.float32).astype(jnp.bfloat16)
    out_grads = jnp.dot(cotangent, output_weight.T, preferred_element_type=jnp.float32).astype(jnp.bfloat16)
    heads_per_group = QUERY_HEADS // KEY_VALUE_HEADS
    score_scale = HEAD_SIZE ** (-0.5)

    def one_head(head_index):
        kv_index = head_index // heads_per_group
        query_head = lax.dynamic_slice_in_dim(queries, head_index * HEAD_SIZE, HEAD_SIZE, 1)
        grad_head = lax.dynamic_slice_in_dim(out_grads, head_index * HEAD_SIZE, HEAD_SIZE, 1)
        key_head = lax.dynamic_slice_in_dim(key_rows, kv_index * HEAD_SIZE, HEAD_SIZE, 1)
        value_head = lax.dynamic_slice_in_dim(value_rows, kv_index * HEAD_SIZE, HEAD_SIZE, 1)
        scores = jnp.dot(query_head, key_head.T, preferred_element_type=jnp.float32) * score_scale
        highest = lax.optimization_barrier(jnp.max(scores, axis=1, keepdims=True))
        weights = jnp.exp(scores - highest)
        totals = lax.optimization_barrier(jnp.sum(weights, axis=1, keepdims=True))
        products = jnp.dot(grad_head, value_head.T, preferred_element_type=jnp.float32)
        drifts = lax.optimization_barrier(jnp.sum(weights * products, axis=1, keepdims=True)) / totals
        softmax_weights = jnp.exp(scores - (highest + jnp.log(totals)))
        slopes = (softmax_weights * (products - drifts) * score_scale).astype(jnp.bfloat16)
        attention = softmax_weights.astype(jnp.bfloat16)
        query_grad = jnp.dot(slopes, key_head, preferred_element_type=jnp.float32)
        key_grad = jnp.dot(slopes.T, query_head, preferred_element_type=jnp.float32)
        value_grad = jnp.dot(attention.T, grad_head, preferred_element_type=jnp.float32)
        return (query_grad, key_grad, value_grad)
    query_grads, key_gradient_rows, value_gradient_rows = lax.map(one_head, jnp.arange(QUERY_HEADS, dtype=jnp.int32))
    query_flat = jnp.transpose(query_grads, (1, 0, 2)).reshape(TGT, QUERY_HEADS * HEAD_SIZE).astype(jnp.bfloat16)
    key_running_sums = lax.optimization_barrier(jnp.sum(key_gradient_rows.reshape(KEY_VALUE_HEADS, heads_per_group, SOURCE_TOTAL, HEAD_SIZE), axis=1))
    value_running_sums = lax.optimization_barrier(jnp.sum(value_gradient_rows.reshape(KEY_VALUE_HEADS, heads_per_group, SOURCE_TOTAL, HEAD_SIZE), axis=1))
    key_flattened = jnp.transpose(key_running_sums, (1, 0, 2)).reshape(SOURCE_TOTAL, KEY_VALUE_HEADS * HEAD_SIZE).astype(jnp.bfloat16)
    value_flattened = jnp.transpose(value_running_sums, (1, 0, 2)).reshape(SOURCE_TOTAL, KEY_VALUE_HEADS * HEAD_SIZE).astype(jnp.bfloat16)
    source_upstream = jnp.dot(key_flattened, key_weight.T, preferred_element_type=jnp.float32) + jnp.dot(value_flattened, value_projection_weight.T, preferred_element_type=jnp.float32)
    source_grad = norm_back(src_scaled, src_inverse, source_gain, source_upstream)
    target_upstream = jnp.dot(query_flat, query_weight.T, preferred_element_type=jnp.float32)
    target_grad = cotangent.astype(jnp.float32) + norm_back(tgt_scaled, tgt_inverse, target_gain, target_upstream)
    key_weight_grad = jnp.dot(src_normed.T, key_flattened, preferred_element_type=jnp.float32)
    return (target_grad, source_grad, key_weight_grad)
```

```python
import functools
from types import SimpleNamespace

import jax
import jax.numpy as jnp
from jax import lax
from jax.experimental import pallas as pl
from jax.experimental.pallas import tpu as pltpu
from jax.sharding import PartitionSpec as P

MESH = pl.DeviceIdType.MESH
HEAD = 256
EPSILON = 1e-05
SCALE = HEAD**-0.5
f32 = jnp.float32
bf16 = jnp.bfloat16
SUBS = 4


def nt(left, right):
    return lax.dot_general(left, right, (((1,), (1,)), ((), ())), preferred_element_type=f32)


def nn(left, right):
    return jnp.dot(left, right, preferred_element_type=f32)


def norm(rows):
    centred = rows - jnp.mean(rows, axis=-1, keepdims=True)
    inverse = lax.rsqrt(jnp.mean(centred * centred, axis=-1, keepdims=True) + EPSILON)
    return centred * inverse, inverse


def norm_back(scaled, inverse, gain, upstream):
    weighted = upstream * gain
    spread = jnp.mean(weighted * scaled, axis=-1, keepdims=True)
    return inverse * (weighted - jnp.mean(weighted, axis=-1, keepdims=True) - scaled * spread)


def loop(start, stop, body):
    lax.fori_loop(start, stop, lambda i, carry: (body(i), carry)[1], 0)


def kernel(names, Z, T, *refs):
    (target_h, source_h, cot_h, tgain, sgain, wq_h, wk_h, wv_h, wo_h, tgrad, sgrad, wgrad) = refs[:12]
    s = SimpleNamespace(**dict(zip(names, refs[12:])))
    D = wq_h.shape[0]
    TR = target_h.shape[0]
    SR = T * source_h.shape[0]
    C = T // 2
    HALF = D // 2
    PART = wk_h.shape[1]
    G = HEAD // PART
    z = lax.axis_index("sp")
    t = lax.axis_index("tp")
    c = lax.rem(t, 2)
    p = lax.div(t, 2)
    other = t + 1 - 2 * c
    j = lax.rem(t, G)

    def remote(src, dst, send, recv, **where):
        return pltpu.make_async_remote_copy(
            src_ref=src, dst_ref=dst, send_sem=send, recv_sem=recv, device_id=where, device_id_type=MESH
        )

    def zat(k):
        return lax.rem(z + k + Z, Z)

    def chip(k):
        return lax.rem(p + k, C)

    def same(k):
        return 2 * chip(k) + c

    def mate(k):
        return t - j + lax.rem(j + k, G)

    row0 = pl.multiple_of(p * (TR // C), TR // C)
    loads = [
        pltpu.make_async_copy(a, b, s.in_sem.at[i])
        for i, (a, b) in enumerate(
            (
                (source_h, s.src),
                (target_h, s.tgt),
                (wq_h, s.wq),
                (cot_h, s.cot),
                (wo_h, s.wo),
                (wk_h, s.wk),
                (wv_h, s.wv),
                (target_h.at[pl.ds(row0, TR // C), :], s.t8),
                (cot_h.at[pl.ds(row0, TR // C), :], s.c8),
            )
        )
    ]
    for one in loads:
        one.start()

    barrier = pltpu.get_barrier_semaphore()

    def greet(**where):
        pl.semaphore_signal(barrier, inc=1, device_id=where, device_id_type=MESH)

    loop(1, Z, lambda k: greet(sp=zat(k)))
    loop(1, C, lambda k: greet(tp=same(k)))
    greet(tp=other)
    greet(tp=mate(2) + 1 - 2 * c)

    loads[0].wait()
    scaled, inverse = norm(s.src[...].astype(f32))
    s.src_scaled[...] = scaled
    s.src_inv[...] = jnp.broadcast_to(inverse, s.src_inv.shape)
    s.g[t] = (scaled * sgain[...]).astype(bf16)
    loads[1].wait()

    def norm_target(i):
        rows = pl.ds(pl.multiple_of(i * 32, 32), 32)
        values, _ = norm(s.tgt[rows, :].astype(f32))
        s.tn[rows, :] = (values * tgain[...]).astype(bf16)

    loop(0, TR // 32, norm_target)
    own = pl.ds(pl.multiple_of(z * TR, TR), TR)
    loads[2].wait()
    s.qd[own, 0:HEAD] = nn(s.tn[...], s.wq[...]).astype(bf16)
    loads[3].wait()
    loads[4].wait()
    s.qd[own, HEAD : 2 * HEAD] = nt(s.cot[...], s.wo[...]).astype(bf16)
    pl.semaphore_wait(barrier, (Z - 1) + (C - 1) + 2)

    def source_copy(k):
        return remote(s.g.at[t], s.g.at[t], s.src_send.at[k], s.src_recv.at[t], tp=same(k))

    loop(1, C, lambda k: source_copy(k).start())

    def forward_copy(k):
        row = s.g.at[same(k)]
        return remote(row, row, s.fwd_send.at[k], s.src_recv.at[same(k)], tp=other)

    forward_copy(0).start()
    rows_sub = TR // SUBS

    def ring_copy(block, sub, way, step):
        rows = s.qd.at[pl.ds(pl.multiple_of(block * TR + sub * rows_sub, rows_sub), rows_sub), :]
        return remote(
            rows, rows, s.ring_send.at[way, step, sub], s.ring_recv.at[way, step, sub],
            sp=zat(1 if way == 0 else -1),
        )

    H = Z // 2

    def reach(way, step):
        if step < H:
            return 0, SUBS
        return (0, SUBS // 2) if way == 0 else (SUBS // 2, SUBS)

    for way in (0, 1):
        loop(*reach(way, 1), lambda sub: ring_copy(z, sub, way, 1).start())

    def ring(step):
        for way in (0, 1):
            block = zat(-step if way == 0 else step)
            lo, hi = reach(way, step)
            flo, fhi = reach(way, step + 1) if step < H else (0, 0)

            def arrive(sub, on):
                ring_copy(block, sub, way, step).wait_recv()
                if on:
                    ring_copy(block, sub, way, step + 1).start()

            if (flo, fhi) == (lo, hi):
                loop(lo, hi, lambda sub: arrive(sub, True))
            else:
                for sub in range(lo, hi):
                    arrive(sub, flo <= sub < fhi)

    loads[5].wait()
    loads[6].wait()

    def join_weights(i):
        rows = pl.ds(pl.multiple_of(i * 256, 256), 256)
        both = jnp.concatenate((s.wk[rows, :].astype(f32), s.wv[rows, :].astype(f32)), axis=1)
        s.wkv[rows, :] = both.astype(bf16)

    loop(0, D // 256, join_weights)

    ring(1)

    def pass_on(k):
        source_copy_from(k).wait_recv()
        forward_copy(k).start()

    def source_copy_from(k):
        row = s.g.at[same(k)]
        return remote(row, row, s.src_send.at[k], s.src_recv.at[same(k)], tp=other)

    loop(1, C, pass_on)
    ring(2)

    def from_other(k):
        at = 2 * chip(k) + 1 - c
        remote(s.g.at[at], s.g.at[at], s.src_send.at[k], s.src_recv.at[at], tp=other).wait_recv()

    loop(0, C, from_other)

    def stack_rows(q):
        both = jnp.concatenate((s.g[2 * q].astype(f32), s.g[2 * q + 1].astype(f32)), axis=0)
        s.rows[pl.ds(pl.multiple_of(q * 16, 16), 16), :] = both.astype(bf16)

    loop(0, C, stack_rows)
    s.kvp[j] = nn(s.rows[...], s.wkv[...]).astype(bf16)

    def join_copy(k):
        return remote(s.kvp.at[j], s.kvp.at[j], s.join_send.at[k], s.join_recv.at[j], tp=mate(k))

    for k in range(1, G):
        join_copy(k).start()
    ring(3)
    for k in range(1, G):
        at = lax.rem(j + k, G)
        remote(s.kvp.at[at], s.kvp.at[at], s.join_send.at[k], s.join_recv.at[at], tp=other).wait_recv()
    parts = [s.kvp[i].astype(f32) for i in range(G)]
    keys = jnp.concatenate([a[:, :PART] for a in parts], axis=1)
    s.keys[...] = keys.astype(bf16)
    s.keys_t[...] = keys.T.astype(bf16)
    s.values[...] = jnp.concatenate([a[:, PART:] for a in parts], axis=1).astype(bf16)

    def block_of(k):
        return zat(lax.div(k + 1, 2) * (2 * lax.rem(k, 2) - 1))

    def stat_copy(k):
        b = block_of(k)
        return remote(s.stat.at[b], s.got.at[z], s.stat_send.at[k], s.stat_recv.at[z], sp=b)

    def scores(k):
        b = block_of(k)
        rows = pl.ds(pl.multiple_of(b * TR, TR), TR)
        scores_t = nt(s.keys[...], s.qd[rows, 0:HEAD]) * SCALE
        products_t = nt(s.values[...], s.qd[rows, HEAD : 2 * HEAD])
        highest = jnp.max(scores_t, axis=0, keepdims=True)
        weights = jnp.exp(scores_t - highest)
        s.e[b] = weights
        s.p[b] = products_t
        s.stat[b, 0:1, :] = highest
        s.stat[b, 1:2, :] = jnp.sum(weights, axis=0, keepdims=True)
        s.stat[b, 2:3, :] = jnp.sum(weights * products_t, axis=0, keepdims=True)
        s.stat[b, 3:4, :] = highest

    def scores_sent(k):
        scores(k)
        stat_copy(k).start()

    ring(4)
    scores(0)
    s.got[z] = s.stat[z]
    loop(1, 3, scores_sent)
    ring(5)
    loop(3, 7, scores_sent)
    ring(6)
    loop(7, 11, scores_sent)
    ring(7)
    loop(11, 15, scores_sent)
    ring(8)
    loop(15, 16, scores_sent)

    def stat_wait(k):
        at = block_of(k)
        remote(s.stat.at[at], s.got.at[at], s.stat_send.at[k], s.stat_recv.at[at], sp=at).wait_recv()

    loop(1, Z, stat_wait)
    top = lax.fori_loop(
        1, Z, lambda i, a: jnp.maximum(a, s.got[i, 0:1, :]), s.got[0, 0:1, :]
    )

    def add_stats(i, sums):
        factor = jnp.exp(s.got[i, 0:1, :] - top)
        return sums[0] + s.got[i, 1:2, :] * factor, sums[1] + s.got[i, 2:3, :] * factor

    total, weighted = lax.fori_loop(0, Z, add_stats, (jnp.zeros_like(top), jnp.zeros_like(top)))
    s.fin[z, 0:1, :] = top + jnp.log(total)
    s.fin[z, 1:2, :] = weighted / total

    def fin_copy(k):
        return remote(s.fin.at[z], s.fin.at[z], s.fin_send.at[k], s.fin_recv.at[z], sp=block_of(k))

    loop(1, Z, lambda k: fin_copy(k).start())

    def fin_wait(k):
        at = block_of(k)
        remote(s.fin.at[at], s.fin.at[at], s.fin_send.at[k], s.fin_recv.at[at], sp=at).wait_recv()

    loop(1, Z, fin_wait)

    def slopes(b):
        cols = pl.ds(pl.multiple_of(b * TR, TR), TR)
        weights = s.e[b] * jnp.exp(s.stat[b, 0:1, :] - s.fin[b, 0:1, :])
        s.att[:, cols] = weights.astype(bf16)
        s.slo[:, cols] = (weights * (s.p[b] - s.fin[b, 1:2, :]) * SCALE).astype(bf16)

    loop(0, Z, slopes)
    s.dq[...] = nn(s.keys_t[...], s.slo[...])

    hd = HEAD // 2

    def hops(way, sub):
        return H if way == sub else H - 1

    def dq_copy(way, step, sub):
        return remote(
            s.dq_out.at[way, step, sub], s.dq_in.at[way, step, sub],
            s.dq_send.at[way, step, sub], s.dq_recv.at[way, step, sub],
            sp=zat(-1 if way == 0 else 1),
        )

    def dq_ring(step):
        for sub in (0, 1):
            for way in (0, 1):
                if step > hops(way, sub):
                    continue
                far = hops(way, sub) + 1 - step
                b = zat(-far if way == 0 else far)
                mine = s.dq[sub * hd : (sub + 1) * hd, pl.ds(pl.multiple_of(b * TR, TR), TR)]
                if step > 1:
                    dq_copy(way, step - 1, sub).wait_recv()
                    mine = mine + s.dq_in[way, step - 1, sub].astype(f32)
                s.dq_out[way, step, sub] = mine.astype(bf16)
                dq_copy(way, step, sub).start()

    dq_ring(1)

    dk = nn(s.slo[...], s.qd[:, 0:HEAD])
    dv = nn(s.att[...], s.qd[:, HEAD : 2 * HEAD])
    for i in range(G):
        cut = slice(i * PART, (i + 1) * PART)
        s.dkv[i] = jnp.concatenate((dk[:, cut], dv[:, cut]), axis=1)
    for k in range(1, G):
        s.dkv_out[k] = s.dkv[lax.rem(j + k, G)].astype(bf16)

    def dkv_copy(k):
        return remote(s.dkv_out.at[k], s.dkv_in.at[k], s.dkv_send.at[k], s.dkv_recv.at[k], tp=mate(k))

    for k in range(1, G):
        dkv_copy(k).start()
    dq_ring(2)
    flat = s.dkv[j]
    for k in range(1, G):
        dkv_copy(k).wait_recv()
        flat = flat + s.dkv_in[k].astype(f32)
    s.flat[...] = flat.astype(bf16)

    part_t = nn(flat.T[:PART, :].astype(bf16), s.rows[...])
    CW = D // Z
    for i in range(Z):
        s.wp[i] = part_t[:, i * CW : (i + 1) * CW].astype(bf16)
    s.wr[z] = s.wp[z]

    def wr_copy(k):
        return remote(s.wp.at[block_of(k)], s.wr.at[z], s.wr_send.at[k], s.wr_recv.at[z], sp=block_of(k))

    loop(1, Z, lambda k: wr_copy(Z - k).start())

    s.su[...] = nt(s.flat[...], s.wkv[...])

    def for_other(q):
        s.ss[q] = s.su[pl.ds(pl.multiple_of(q * 16 + 8 * (1 - c), 8), 8), :].astype(bf16)

    loop(0, C, for_other)
    su_pair = remote(s.ss, s.sr, s.pair_send.at[0], s.pair_recv.at[0], tp=other)
    su_pair.start()
    dq_ring(3)
    su_pair.wait_recv()

    def sw_copy(k):
        return remote(s.sv.at[chip(k)], s.sw.at[p], s.sw_send.at[k], s.sw_recv.at[p], tp=same(k))

    def both_cores(k):
        q = chip(k)
        mine = s.su[pl.ds(pl.multiple_of(q * 16 + 8 * c, 8), 8), :]
        return (mine + s.sr[q].astype(f32)).astype(bf16)

    s.sw[p] = both_cores(0)

    def sw_start(k):
        s.sv[chip(k)] = both_cores(k)
        sw_copy(k).start()

    loop(1, C, sw_start)
    dq_ring(4)
    dq_ring(5)

    def wr_wait(k):
        at = block_of(k)
        remote(s.wp.at[at], s.wr.at[at], s.wr_send.at[k], s.wr_recv.at[at], sp=at).wait_recv()

    loop(1, Z, wr_wait)
    s.wf[z] = lax.fori_loop(
        1, Z, lambda i, a: a + s.wr[i].astype(f32), s.wr[0].astype(f32)
    ).astype(bf16)

    def wf_copy(k):
        return remote(s.wf.at[z], s.wf.at[z], s.wf_send.at[k], s.wf_recv.at[z], sp=block_of(k))

    loop(1, Z, lambda k: wf_copy(Z - k).start())
    dq_ring(6)

    def sw_wait(k):
        at = chip(k)
        remote(s.sv.at[at], s.sw.at[at], s.sw_send.at[k], s.sw_recv.at[at], tp=other).wait_recv()

    loop(1, C, sw_wait)
    s.su8[...] = s.sw[0].astype(f32)

    def add_sw(i):
        s.su8[...] += s.sw[i].astype(f32)

    loop(1, C, add_sw)
    sgrad[...] = norm_back(s.src_scaled[...], s.src_inv[:, 0:1], sgain[...], s.su8[...])
    dq_ring(7)
    dq_ring(8)
    halves = []
    for sub in (0, 1):
        mine = s.dq[sub * hd : (sub + 1) * hd, own]
        for way in (0, 1):
            last = hops(way, sub)
            dq_copy(way, last, sub).wait_recv()
            mine = mine + s.dq_in[way, last, sub].astype(f32)
        halves.append(mine)
    query_flat = jnp.concatenate(halves, axis=0).T.astype(bf16)

    TB = TR // C

    def half_cols(h):
        return s.wq[pl.ds(pl.multiple_of(h * HALF, HALF), HALF), :]

    s.tsend[...] = nt(query_flat, half_cols(1 - c)).reshape(C, TB, HALF).astype(bf16)
    tu_pair = remote(s.tsend, s.trecv, s.pair_send.at[1], s.pair_recv.at[1], tp=other)
    tu_pair.start()
    s.tmine[...] = nt(query_flat, half_cols(c)).reshape(C, TB, HALF)
    tu_pair.wait_recv()

    def tw_copy(k):
        return remote(s.tv.at[chip(k)], s.tw.at[p], s.tw_send.at[k], s.tw_recv.at[p], tp=same(k))

    def tboth(k):
        q = chip(k)
        return (s.tmine[q] + s.trecv[q].astype(f32)).astype(bf16)

    s.tw[p] = tboth(0)

    def tw_start(k):
        s.tv[chip(k)] = tboth(k)
        tw_copy(k).start()

    loop(1, C, tw_start)

    def wf_wait(k):
        at = block_of(k)
        remote(s.wf.at[at], s.wf.at[at], s.wf_send.at[k], s.wf_recv.at[at], sp=at).wait_recv()

    loop(1, Z, wf_wait)

    def put_weight(i):
        wgrad[pl.ds(pl.multiple_of(i * CW, CW), CW), :] = s.wf[i].astype(f32).T

    loop(0, Z, put_weight)

    def tw_wait(k):
        at = chip(k)
        remote(s.tv.at[at], s.tw.at[at], s.tw_send.at[k], s.tw_recv.at[at], tp=other).wait_recv()

    loop(1, C, tw_wait)
    s.tu8[...] = s.tw[0].astype(f32)

    def add_tw(i):
        s.tu8[...] += s.tw[i].astype(f32)

    loop(1, C, add_tw)
    TO = TB // 2
    lower, upper = s.tu8[0:TO, :], s.tu8[TO:TB, :]
    mine = jnp.where(c == 0, lower, upper)
    s.tx_out[...] = jnp.where(c == 0, upper, lower)
    last_pair = remote(s.tx_out, s.tx_in, s.pair_send.at[2], s.pair_recv.at[2], tp=other)
    last_pair.start()
    loads[7].wait()
    loads[8].wait()
    scaled, inverse = norm(s.t8[...].astype(f32))
    cot = s.c8[...].astype(f32)
    scaled = jnp.where(c == 0, scaled[0:TO], scaled[TO:TB])
    inverse = jnp.where(c == 0, inverse[0:TO], inverse[TO:TB])
    cot = jnp.where(c == 0, cot[0:TO], cot[TO:TB])
    last_pair.wait_recv()
    theirs = s.tx_in[...]
    upstream = jnp.concatenate(
        (jnp.where(c == 0, mine, theirs), jnp.where(c == 0, theirs, mine)), axis=1
    )
    tgrad[...] = cot + norm_back(scaled, inverse, tgain[...], upstream)

    loop(1, C, lambda k: source_copy(k).wait_send())
    loop(0, C, lambda k: forward_copy(k).wait_send())
    for way in (0, 1):
        for step in range(1, H + 1):
            block = zat(-(step - 1) if way == 0 else step - 1)
            loop(*reach(way, step), lambda sub: ring_copy(block, sub, way, step).wait_send())
    for k in range(1, G):
        join_copy(k).wait_send()
        dkv_copy(k).wait_send()

    def line_sends(k):
        stat_copy(k).wait_send()
        fin_copy(k).wait_send()
        wr_copy(k).wait_send()
        wf_copy(k).wait_send()

    loop(1, Z, line_sends)
    for way in (0, 1):
        for sub in (0, 1):
            for step in range(1, hops(way, sub) + 1):
                dq_copy(way, step, sub).wait_send()

    def plane_sends(k):
        sw_copy(k).wait_send()
        tw_copy(k).wait_send()

    loop(1, C, plane_sends)
    su_pair.wait_send()
    tu_pair.wait_send()
    last_pair.wait_send()


def solution(mesh):
    Z, T = mesh.shape["sp"], mesh.shape["tp"]

    def on_device(target, source, cotangent, target_gain, source_gain, wq, wk, wv, wo):
        TR, D = target.shape
        SB = source.shape[0]
        SR = SB * T
        C = T // 2
        PART = wk.shape[1]
        G = HEAD // PART
        H = Z // 2
        TB = TR // C
        CW = D // Z
        V = pltpu.VMEM
        dma = pltpu.SemaphoreType.DMA
        scratch = dict(
            src=V((SB, D), bf16), tgt=V((TR, D), bf16), cot=V((TR, D), bf16),
            wq=V((D, HEAD), bf16), wk=V((D, PART), bf16), wv=V((D, PART), bf16), wo=V((HEAD, D), bf16),
            t8=V((TB, D), bf16), c8=V((TB, D), bf16),
            src_scaled=V((SB, D), f32), src_inv=V((SB, 128), f32),
            g=V((T, SB, D), bf16), tn=V((TR, D), bf16), qd=V((Z * TR, 2 * HEAD), bf16),
            wkv=V((D, 2 * PART), bf16), rows=V((SR, D), bf16), kvp=V((G, SR, 2 * PART), bf16),
            keys=V((SR, HEAD), bf16), keys_t=V((HEAD, SR), bf16), values=V((SR, HEAD), bf16),
            e=V((Z, SR, TR), f32), p=V((Z, SR, TR), f32),
            stat=V((Z, 4, TR), f32), got=V((Z, 4, TR), f32), fin=V((Z, 2, TR), f32),
            att=V((SR, Z * TR), bf16), slo=V((SR, Z * TR), bf16), dq=V((HEAD, Z * TR), f32),
            dq_out=V((2, H + 1, 2, HEAD // 2, TR), bf16), dq_in=V((2, H + 1, 2, HEAD // 2, TR), bf16),
            dkv=V((G, SR, 2 * PART), f32), dkv_out=V((G, SR, 2 * PART), bf16), dkv_in=V((G, SR, 2 * PART), bf16),
            flat=V((SR, 2 * PART), bf16),
            wp=V((Z, PART, CW), bf16), wr=V((Z, PART, CW), bf16), wf=V((Z, PART, CW), bf16),
            su=V((SR, D), f32), ss=V((C, SB, D), bf16), sr=V((C, SB, D), bf16),
            sv=V((C, SB, D), bf16), sw=V((C, SB, D), bf16), su8=V((SB, D), f32),
            tsend=V((C, TB, D // 2), bf16), trecv=V((C, TB, D // 2), bf16), tmine=V((C, TB, D // 2), f32),
            tv=V((C, TB, D // 2), bf16), tw=V((C, TB, D // 2), bf16), tu8=V((TB, D // 2), f32),
            tx_out=V((TB // 2, D // 2), f32), tx_in=V((TB // 2, D // 2), f32),
            in_sem=dma((9,)), src_send=dma((C,)), fwd_send=dma((C,)), src_recv=dma((T,)),
            ring_send=dma((2, H + 1, SUBS)), ring_recv=dma((2, H + 1, SUBS)),
            join_send=dma((G,)), join_recv=dma((G,)), dkv_send=dma((G,)), dkv_recv=dma((G,)),
            stat_send=dma((Z,)), stat_recv=dma((Z,)), fin_send=dma((Z,)), fin_recv=dma((Z,)),
            wr_send=dma((Z,)), wr_recv=dma((Z,)), wf_send=dma((Z,)), wf_recv=dma((Z,)),
            dq_send=dma((2, H + 1, 2)), dq_recv=dma((2, H + 1, 2)),
            sw_send=dma((C,)), sw_recv=dma((C,)), tw_send=dma((C,)), tw_recv=dma((C,)),
            pair_send=dma((3,)), pair_recv=dma((3,)),
        )
        vmem = pl.BlockSpec(memory_space=pltpu.VMEM)
        any_ = pl.BlockSpec(memory_space=pl.ANY)
        return pl.pallas_call(
            functools.partial(kernel, tuple(scratch), Z, T),
            out_shape=(
                jax.ShapeDtypeStruct((TR // T, D), f32),
                jax.ShapeDtypeStruct((SB, D), f32),
                jax.ShapeDtypeStruct((D, PART), f32),
            ),
            in_specs=[any_, any_, any_, vmem, vmem, any_, any_, any_, any_],
            out_specs=(vmem, vmem, vmem),
            scratch_shapes=list(scratch.values()),
            compiler_params=pltpu.CompilerParams(
                collective_id=0, has_side_effects=True, vmem_limit_bytes=62 * 1024 * 1024
            ),
            name="backward",
        )(target, source, cotangent, target_gain.reshape(1, D), source_gain.reshape(1, D), wq, wk, wv, wo)

    return jax.shard_map(
        on_device,
        mesh=mesh,
        in_specs=(
            P("sp", None), P(("sp", "tp"), None), P("sp", None), P(), P(),
            P(None, "tp"), P(None, "tp"), P(None, "tp"), P("tp", None),
        ),
        out_specs=(P(("sp", "tp"), None), P(("sp", "tp"), None), P(None, "tp")),
        check_vma=False,
    )
```

```python
import functools
from types import SimpleNamespace

import jax
import jax.numpy as jnp
from jax import lax
from jax.experimental import pallas as pl
from jax.experimental.pallas import tpu as pltpu
from jax.sharding import PartitionSpec as P

MESH = pl.DeviceIdType.MESH
HEAD = 256
EPSILON = 1e-05
SCALE = HEAD**-0.5
f32 = jnp.float32
bf16 = jnp.bfloat16
SUBS = 4


def nt(left, right):
    return lax.dot_general(left, right, (((1,), (1,)), ((), ())), preferred_element_type=f32)


def nn(left, right):
    return jnp.dot(left, right, preferred_element_type=f32)


def norm(rows):
    centred = rows - jnp.mean(rows, axis=-1, keepdims=True)
    inverse = lax.rsqrt(jnp.mean(centred * centred, axis=-1, keepdims=True) + EPSILON)
    return centred * inverse, inverse


def norm_back(scaled, inverse, gain, upstream):
    weighted = upstream * gain
    spread = jnp.mean(weighted * scaled, axis=-1, keepdims=True)
    return inverse * (weighted - jnp.mean(weighted, axis=-1, keepdims=True) - scaled * spread)


def loop(start, stop, body):
    lax.fori_loop(start, stop, lambda i, carry: (body(i), carry)[1], 0)


def kernel(names, Z, T, *refs):
    (target_h, source_h, cot_h, tgain, sgain, wq_h, wk_h, wv_h, wo_h, tgrad, sgrad, wgrad) = refs[:12]
    s = SimpleNamespace(**dict(zip(names, refs[12:])))
    D = wq_h.shape[0]
    TR = target_h.shape[0]
    SR = T * source_h.shape[0]
    C = T // 2
    HALF = D // 2
    PART = wk_h.shape[0]
    G = HEAD // PART
    z = lax.axis_index("sp")
    t = lax.axis_index("tp")
    c = lax.rem(t, 2)
    p = lax.div(t, 2)
    other = t + 1 - 2 * c
    j = lax.rem(t, G)

    def remote(src, dst, send, recv, **where):
        return pltpu.make_async_remote_copy(
            src_ref=src, dst_ref=dst, send_sem=send, recv_sem=recv, device_id=where, device_id_type=MESH
        )

    def zat(k):
        return lax.rem(z + k + Z, Z)

    def chip(k):
        return lax.rem(p + k, C)

    def same(k):
        return 2 * chip(k) + c

    def mate(k):
        return t - j + lax.rem(j + k, G)

    row0 = pl.multiple_of(p * (TR // C), TR // C)
    loads = [
        pltpu.make_async_copy(a, b, s.in_sem.at[i])
        for i, (a, b) in enumerate(
            (
                (source_h, s.src),
                (target_h, s.tgt),
                (wq_h, s.wq),
                (cot_h, s.cot),
                (wo_h, s.wo),
                (wk_h, s.wkv.at[0:PART, :]),
                (wv_h, s.wkv.at[PART : 2 * PART, :]),
                (target_h.at[pl.ds(row0, TR // C), :], s.t8),
                (cot_h.at[pl.ds(row0, TR // C), :], s.c8),
            )
        )
    ]
    for one in loads:
        one.start()

    barrier = pltpu.get_barrier_semaphore()

    def greet(**where):
        pl.semaphore_signal(barrier, inc=1, device_id=where, device_id_type=MESH)

    loop(1, Z, lambda k: greet(sp=zat(k)))
    loop(1, C, lambda k: greet(tp=same(k)))
    greet(tp=other)
    greet(tp=mate(2) + 1 - 2 * c)

    loads[0].wait()
    scaled, inverse = norm(s.src[...].astype(f32))
    s.src_scaled[...] = scaled
    s.src_inv[...] = jnp.broadcast_to(inverse, s.src_inv.shape)
    s.g[t] = (scaled * sgain[...]).astype(bf16)
    loads[1].wait()

    def norm_target(i):
        rows = pl.ds(pl.multiple_of(i * 32, 32), 32)
        values, _ = norm(s.tgt[rows, :].astype(f32))
        s.tn[rows, :] = (values * tgain[...]).astype(bf16)

    loop(0, TR // 32, norm_target)
    own = pl.ds(pl.multiple_of(z * TR, TR), TR)
    loads[2].wait()
    s.qd[own, 0:HEAD] = nn(s.tn[...], s.wq[...]).astype(bf16)
    loads[3].wait()
    loads[4].wait()
    s.qd[own, HEAD : 2 * HEAD] = nt(s.cot[...], s.wo[...]).astype(bf16)
    pl.semaphore_wait(barrier, (Z - 1) + (C - 1) + 2)

    def source_copy(k):
        return remote(s.g.at[t], s.g.at[t], s.src_send.at[k], s.src_recv.at[t], tp=same(k))

    loop(1, C, lambda k: source_copy(k).start())

    def forward_copy(k):
        row = s.g.at[same(k)]
        return remote(row, row, s.fwd_send.at[k], s.src_recv.at[same(k)], tp=other)

    forward_copy(0).start()
    rows_sub = TR // SUBS

    def ring_copy(block, sub, way, step):
        rows = s.qd.at[pl.ds(pl.multiple_of(block * TR + sub * rows_sub, rows_sub), rows_sub), :]
        return remote(
            rows, rows, s.ring_send.at[way, step, sub], s.ring_recv.at[way, step, sub],
            sp=zat(1 if way == 0 else -1),
        )

    H = Z // 2

    def reach(way, step):
        if step < H:
            return 0, SUBS
        return (0, SUBS // 2) if way == 0 else (SUBS // 2, SUBS)

    for way in (0, 1):
        loop(*reach(way, 1), lambda sub: ring_copy(z, sub, way, 1).start())

    def ring(step, first=-1):
        def arrive(way, sub, on):
            block = zat(-step if way == 0 else step)
            ring_copy(block, sub, way, step).wait_recv()
            if on:
                ring_copy(block, sub, way, step + 1).start()

        def both(lo, hi, on):
            def at(sub):
                arrive(0, sub, on[0])
                arrive(1, sub, on[1])
                if first >= 0:
                    scores_sent(first + sub)

            loop(lo, hi, at)

        if step < H - 1:
            both(0, SUBS, (True, True))
        elif step == H - 1:
            both(0, SUBS // 2, (True, False))
            both(SUBS // 2, SUBS, (False, True))
        else:

            def last(sub):
                arrive(0, sub, False)
                arrive(1, SUBS // 2 + sub, False)
                if first >= 0:
                    scores_sent(first + sub)

            loop(0, SUBS // 2, last)

    loads[5].wait()
    loads[6].wait()

    ring(1)

    def pass_on(k):
        source_copy_from(k).wait_recv()
        forward_copy(k).start()

    def source_copy_from(k):
        row = s.g.at[same(k)]
        return remote(row, row, s.src_send.at[k], s.src_recv.at[same(k)], tp=other)

    loop(1, C, pass_on)
    ring(2)

    def from_other(k):
        at = 2 * chip(k) + 1 - c
        remote(s.g.at[at], s.g.at[at], s.src_send.at[k], s.src_recv.at[at], tp=other).wait_recv()

    loop(0, C, from_other)

    def stack_rows(q):
        both = jnp.concatenate((s.g[2 * q].astype(f32), s.g[2 * q + 1].astype(f32)), axis=0)
        s.rows[pl.ds(pl.multiple_of(q * 16, 16), 16), :] = both.astype(bf16)

    loop(0, C, stack_rows)
    s.kvp[j] = nt(s.rows[...], s.wkv[...]).astype(bf16)

    def join_copy(k):
        return remote(s.kvp.at[j], s.kvp.at[j], s.join_send.at[k], s.join_recv.at[j], tp=mate(k))

    for k in range(1, G):
        join_copy(k).start()
    ring(3)
    ring(4)
    for k in range(1, G):
        at = lax.rem(j + k, G)
        remote(s.kvp.at[at], s.kvp.at[at], s.join_send.at[k], s.join_recv.at[at], tp=other).wait_recv()
    parts = [s.kvp[i].astype(f32) for i in range(G)]
    keys = jnp.concatenate([a[:, :PART] for a in parts], axis=1)
    s.keys[...] = keys.astype(bf16)
    s.keys_t[...] = keys.T.astype(bf16)
    s.values[...] = jnp.concatenate([a[:, PART:] for a in parts], axis=1).astype(bf16)

    def block_of(k):
        return zat(lax.div(k + 1, 2) * (2 * lax.rem(k, 2) - 1))

    def stat_copy(k):
        b = block_of(k)
        return remote(s.stat.at[b], s.got.at[z], s.stat_send.at[k], s.stat_recv.at[z], sp=lax.rem(b + H, Z))

    def scores(k):
        b = block_of(k)
        rows = pl.ds(pl.multiple_of(b * TR, TR), TR)
        scores_t = nt(s.keys[...], s.qd[rows, 0:HEAD]) * SCALE
        products_t = nt(s.values[...], s.qd[rows, HEAD : 2 * HEAD])
        highest = jnp.max(scores_t, axis=0, keepdims=True)
        weights = jnp.exp(scores_t - highest)
        s.e[b] = weights
        s.p[b] = products_t
        s.stat[b, 0:1, :] = highest
        s.stat[b, 1:2, :] = jnp.sum(weights, axis=0, keepdims=True)
        s.stat[b, 2:3, :] = jnp.sum(weights * products_t, axis=0, keepdims=True)
        s.stat[b, 3:4, :] = highest

    def scores_sent(k):
        scores(k)
        stat_copy(k).start()

    ring(5, 0)
    ring(6, 4)
    ring(7, 8)
    ring(8, 12)
    loop(14, 15, scores_sent)
    scores(15)
    far = zat(H)
    s.got[z] = s.stat[far]

    def stat_wait(k):
        at = block_of(k)
        remote(s.stat.at[at], s.got.at[at], s.stat_send.at[k], s.stat_recv.at[at], sp=at).wait_recv()

    loop(1, Z, stat_wait)
    top = lax.fori_loop(
        1, Z, lambda i, a: jnp.maximum(a, s.got[i, 0:1, :]), s.got[0, 0:1, :]
    )

    def add_stats(i, sums):
        factor = jnp.exp(s.got[i, 0:1, :] - top)
        return sums[0] + s.got[i, 1:2, :] * factor, sums[1] + s.got[i, 2:3, :] * factor

    total, weighted = lax.fori_loop(0, Z, add_stats, (jnp.zeros_like(top), jnp.zeros_like(top)))
    s.fin[far, 0:1, :] = top + jnp.log(total)
    s.fin[far, 1:2, :] = weighted / total

    def fin_copy(k):
        return remote(s.fin.at[far], s.fin.at[far], s.fin_send.at[k], s.fin_recv.at[far], sp=block_of(k))

    loop(1, Z, lambda k: fin_copy(Z - k).start())

    def fin_wait(k):
        at = block_of(k - 1)
        remote(s.fin.at[at], s.fin.at[at], s.fin_send.at[k], s.fin_recv.at[at], sp=at).wait_recv()

    loop(1, Z, fin_wait)

    def slopes(b):
        cols = pl.ds(pl.multiple_of(b * TR, TR), TR)
        weights = s.e[b] * jnp.exp(s.stat[b, 0:1, :] - s.fin[b, 0:1, :])
        s.att[:, cols] = weights.astype(bf16)
        s.slo[:, cols] = (weights * (s.p[b] - s.fin[b, 1:2, :]) * SCALE).astype(bf16)

    loop(0, Z, slopes)
    s.dq[...] = nn(s.keys_t[...], s.slo[...])

    hd = HEAD // 2

    def hops(way, sub):
        return H if way == sub else H - 1

    def dq_copy(way, step, sub):
        return remote(
            s.dq_out.at[way, step, sub], s.dq_in.at[way, step, sub],
            s.dq_send.at[way, step, sub], s.dq_recv.at[way, step, sub],
            sp=zat(-1 if way == 0 else 1),
        )

    def dq_ring(step):
        for sub in (0, 1):
            for way in (0, 1):
                if step > hops(way, sub):
                    continue
                far = hops(way, sub) + 1 - step
                b = zat(-far if way == 0 else far)
                mine = s.dq[sub * hd : (sub + 1) * hd, pl.ds(pl.multiple_of(b * TR, TR), TR)]
                if step > 1:
                    dq_copy(way, step - 1, sub).wait_recv()
                    mine = mine + s.dq_in[way, step - 1, sub].astype(f32)
                s.dq_out[way, step, sub] = mine.astype(bf16)
                dq_copy(way, step, sub).start()

    dq_ring(1)

    dk = nn(s.slo[...], s.qd[:, 0:HEAD])
    dv = nn(s.att[...], s.qd[:, HEAD : 2 * HEAD])
    for i in range(G):
        cut = slice(i * PART, (i + 1) * PART)
        s.dkv[i] = jnp.concatenate((dk[:, cut], dv[:, cut]), axis=1)
    for k in range(1, G):
        s.dkv_out[k] = s.dkv[lax.rem(j + k, G)].astype(bf16)

    def dkv_copy(k):
        return remote(s.dkv_out.at[k], s.dkv_in.at[k], s.dkv_send.at[k], s.dkv_recv.at[k], tp=mate(k))

    for k in range(1, G):
        dkv_copy(k).start()
    dq_ring(2)
    dq_ring(3)
    flat = s.dkv[j]
    for k in range(1, G):
        dkv_copy(k).wait_recv()
        flat = flat + s.dkv_in[k].astype(f32)
    s.flat[...] = flat.astype(bf16)

    part_t = nn(flat.T[:PART, :].astype(bf16), s.rows[...])
    CW = D // Z
    for i in range(Z):
        s.wp[i] = part_t[:, i * CW : (i + 1) * CW].astype(bf16)
    R = H // 2

    def sign(way, k):
        return zat(k if way == 1 else -k)

    def w_copy(way, k):
        hop = k % R or R
        src = s.w_rel.at[way] if k == R else s.wp.at[sign(way, k)]
        return remote(src, s.w_in.at[way, k], s.w_send.at[way, k], s.w_recv.at[way, k], sp=sign(way, hop))

    top_hop = (2 * R, 2 * R - 1)
    for way in (0, 1):
        for k in range(top_hop[way], 0, -1):
            if k != R:
                w_copy(way, k).start()

    def w_relay():
        for way in (0, 1):
            total = s.wp[sign(way, R)].astype(f32)
            for k in range(R + 1, top_hop[way] + 1):
                w_copy(way, k).wait_recv()
                total = total + s.w_in[way, k].astype(f32)
            s.w_rel[way] = total.astype(bf16)
            w_copy(way, R).start()

    def f_copy(way, k, relay):
        block = sign(1 - way, R) if relay else z
        hop = k - R if relay else k
        return remote(s.wf.at[block], s.wf.at[block], s.f_send.at[way, k], s.f_recv.at[block], sp=sign(way, hop))

    def w_owner():
        total = s.wp[z].astype(f32)
        for way in (0, 1):
            for k in range(1, R + 1):
                w_copy(way, k).wait_recv()
                total = total + s.w_in[way, k].astype(f32)
        s.wf[z] = total.astype(bf16)
        for way in (0, 1):
            for k in range(R, 0, -1):
                f_copy(way, k, False).start()

    def f_wait(k):
        at = block_of(k)
        remote(s.wf.at[at], s.wf.at[at], s.f_send.at[0, k % 2], s.f_recv.at[at], sp=at).wait_recv()

    def f_relay():
        for way in (0, 1):
            f_wait(2 * R - 1 if way == 0 else 2 * R)
            for k in range(top_hop[way], R, -1):
                f_copy(way, k, True).start()

    dq_ring(4)
    s.su[...] = nn(s.flat[...], s.wkv[...])

    def for_other(q):
        s.ss[q] = s.su[pl.ds(pl.multiple_of(q * 16 + 8 * (1 - c), 8), 8), :].astype(bf16)

    loop(0, C, for_other)
    su_pair = remote(s.ss, s.sr, s.pair_send.at[0], s.pair_recv.at[0], tp=other)
    su_pair.start()
    dq_ring(5)
    su_pair.wait_recv()

    def sw_copy(k):
        return remote(s.sv.at[chip(k)], s.sw.at[p], s.sw_send.at[k], s.sw_recv.at[p], tp=same(k))

    def both_cores(k):
        q = chip(k)
        mine = s.su[pl.ds(pl.multiple_of(q * 16 + 8 * c, 8), 8), :]
        return (mine + s.sr[q].astype(f32)).astype(bf16)

    s.sw[p] = both_cores(0)

    def sw_start(k):
        s.sv[chip(k)] = both_cores(k)
        sw_copy(k).start()

    loop(1, C, sw_start)
    dq_ring(6)
    w_relay()
    dq_ring(7)
    dq_ring(8)
    w_owner()
    halves = []
    for sub in (0, 1):
        mine = s.dq[sub * hd : (sub + 1) * hd, own]
        for way in (0, 1):
            last = hops(way, sub)
            dq_copy(way, last, sub).wait_recv()
            mine = mine + s.dq_in[way, last, sub].astype(f32)
        halves.append(mine)
    query_flat = jnp.concatenate(halves, axis=0).T.astype(bf16)

    TB = TR // C

    def half_cols(h):
        return s.wq[pl.ds(pl.multiple_of(h * HALF, HALF), HALF), :]

    s.tsend[...] = nt(query_flat, half_cols(1 - c)).reshape(C, TB, HALF).astype(bf16)
    tu_pair = remote(s.tsend, s.trecv, s.pair_send.at[1], s.pair_recv.at[1], tp=other)
    tu_pair.start()
    s.tmine[...] = nt(query_flat, half_cols(c)).reshape(C, TB, HALF)

    def sw_wait(k):
        at = chip(k)
        remote(s.sv.at[at], s.sw.at[at], s.sw_send.at[k], s.sw_recv.at[at], tp=other).wait_recv()

    tu_pair.wait_recv()

    def tw_copy(k):
        return remote(s.tv.at[chip(k)], s.tw.at[p], s.tw_send.at[k], s.tw_recv.at[p], tp=same(k))

    def tboth(k):
        q = chip(k)
        return (s.tmine[q] + s.trecv[q].astype(f32)).astype(bf16)

    s.tw[p] = tboth(0)

    def tw_start(k):
        s.tv[chip(k)] = tboth(k)
        tw_copy(k).start()

    loop(1, C, tw_start)

    loop(1, C, sw_wait)
    s.su8[...] = s.sw[0].astype(f32)

    def add_sw(i):
        s.su8[...] += s.sw[i].astype(f32)

    loop(1, C, add_sw)
    sgrad[...] = norm_back(s.src_scaled[...], s.src_inv[:, 0:1], sgain[...], s.su8[...])
    f_relay()
    loop(1, C, lambda k: source_copy(k).wait_send())
    loop(0, C, lambda k: forward_copy(k).wait_send())
    for way in (0, 1):
        for step in range(1, H + 1):
            block = zat(-(step - 1) if way == 0 else step - 1)
            loop(*reach(way, step), lambda sub: ring_copy(block, sub, way, step).wait_send())
    for k in range(1, G):
        join_copy(k).wait_send()
        dkv_copy(k).wait_send()

    def line_sends(k):
        stat_copy(k - 1).wait_send()
        fin_copy(k).wait_send()

    loop(1, Z, line_sends)
    for way in (0, 1):
        for sub in (0, 1):
            for step in range(1, hops(way, sub) + 1):
                dq_copy(way, step, sub).wait_send()
        for k in range(1, top_hop[way] + 1):
            w_copy(way, k).wait_send()
    su_pair.wait_send()
    loop(1, C, lambda k: sw_copy(k).wait_send())

    def tw_wait(k):
        at = chip(k)
        remote(s.tv.at[at], s.tw.at[at], s.tw_send.at[k], s.tw_recv.at[at], tp=other).wait_recv()

    loop(1, C, tw_wait)
    s.tu8[...] = s.tw[0].astype(f32)

    def add_tw(i):
        s.tu8[...] += s.tw[i].astype(f32)

    loop(1, C, add_tw)
    TO = TB // 2
    lower, upper = s.tu8[0:TO, :], s.tu8[TO:TB, :]
    mine = jnp.where(c == 0, lower, upper)
    s.tx_out[...] = jnp.where(c == 0, upper, lower)
    last_pair = remote(s.tx_out, s.tx_in, s.pair_send.at[2], s.pair_recv.at[2], tp=other)
    last_pair.start()
    loads[7].wait()
    loads[8].wait()
    scaled, inverse = norm(s.t8[...].astype(f32))
    cot = s.c8[...].astype(f32)
    scaled = jnp.where(c == 0, scaled[0:TO], scaled[TO:TB])
    inverse = jnp.where(c == 0, inverse[0:TO], inverse[TO:TB])
    cot = jnp.where(c == 0, cot[0:TO], cot[TO:TB])
    last_pair.wait_recv()
    theirs = s.tx_in[...]
    upstream = jnp.concatenate(
        (jnp.where(c == 0, mine, theirs), jnp.where(c == 0, theirs, mine)), axis=1
    )
    tgrad[...] = cot + norm_back(scaled, inverse, tgain[...], upstream)

    for k in range(1, Z):
        if k not in (2 * R - 1, 2 * R):
            f_wait(k)
    for i in range(Z):
        wgrad[:, i * CW : (i + 1) * CW] = s.wf[i].astype(f32)
    for way in (0, 1):
        for k in range(1, top_hop[way] + 1):
            f_copy(way, k, k > R).wait_send()
    loop(1, C, lambda k: tw_copy(k).wait_send())
    tu_pair.wait_send()
    last_pair.wait_send()


def solution(mesh):
    Z, T = mesh.shape["sp"], mesh.shape["tp"]

    def on_device(target, source, cotangent, target_gain, source_gain, wq, wk, wv, wo):
        TR, D = target.shape
        SB = source.shape[0]
        SR = SB * T
        C = T // 2
        PART = wk.shape[1]
        G = HEAD // PART
        H = Z // 2
        TB = TR // C
        CW = D // Z
        V = pltpu.VMEM
        dma = pltpu.SemaphoreType.DMA
        scratch = dict(
            src=V((SB, D), bf16), tgt=V((TR, D), bf16), cot=V((TR, D), bf16),
            wq=V((D, HEAD), bf16), wo=V((HEAD, D), bf16),
            t8=V((TB, D), bf16), c8=V((TB, D), bf16),
            src_scaled=V((SB, D), f32), src_inv=V((SB, 128), f32),
            g=V((T, SB, D), bf16), tn=V((TR, D), bf16), qd=V((Z * TR, 2 * HEAD), bf16),
            wkv=V((2 * PART, D), bf16), rows=V((SR, D), bf16), kvp=V((G, SR, 2 * PART), bf16),
            keys=V((SR, HEAD), bf16), keys_t=V((HEAD, SR), bf16), values=V((SR, HEAD), bf16),
            e=V((Z, SR, TR), f32), p=V((Z, SR, TR), f32),
            stat=V((Z, 4, TR), f32), got=V((Z, 4, TR), f32), fin=V((Z, 2, TR), f32),
            att=V((SR, Z * TR), bf16), slo=V((SR, Z * TR), bf16), dq=V((HEAD, Z * TR), f32),
            dq_out=V((2, H + 1, 2, HEAD // 2, TR), bf16), dq_in=V((2, H + 1, 2, HEAD // 2, TR), bf16),
            dkv=V((G, SR, 2 * PART), f32), dkv_out=V((G, SR, 2 * PART), bf16), dkv_in=V((G, SR, 2 * PART), bf16),
            flat=V((SR, 2 * PART), bf16),
            wp=V((Z, PART, CW), bf16), w_in=V((2, H + 1, PART, CW), bf16), w_rel=V((2, PART, CW), bf16),
            wf=V((Z, PART, CW), bf16),
            su=V((SR, D), f32), ss=V((C, SB, D), bf16), sr=V((C, SB, D), bf16),
            sv=V((C, SB, D), bf16), sw=V((C, SB, D), bf16), su8=V((SB, D), f32),
            tsend=V((C, TB, D // 2), bf16), trecv=V((C, TB, D // 2), bf16), tmine=V((C, TB, D // 2), f32),
            tv=V((C, TB, D // 2), bf16), tw=V((C, TB, D // 2), bf16), tu8=V((TB, D // 2), f32),
            tx_out=V((TB // 2, D // 2), f32), tx_in=V((TB // 2, D // 2), f32),
            in_sem=dma((9,)), src_send=dma((C,)), fwd_send=dma((C,)), src_recv=dma((T,)),
            ring_send=dma((2, H + 1, SUBS)), ring_recv=dma((2, H + 1, SUBS)),
            join_send=dma((G,)), join_recv=dma((G,)), dkv_send=dma((G,)), dkv_recv=dma((G,)),
            stat_send=dma((Z,)), stat_recv=dma((Z,)), fin_send=dma((Z,)), fin_recv=dma((Z,)),
            w_send=dma((2, H + 1)), w_recv=dma((2, H + 1)), f_send=dma((2, H + 1)), f_recv=dma((Z,)),
            dq_send=dma((2, H + 1, 2)), dq_recv=dma((2, H + 1, 2)),
            sw_send=dma((C,)), sw_recv=dma((C,)), tw_send=dma((C,)), tw_recv=dma((C,)),
            pair_send=dma((3,)), pair_recv=dma((3,)),
        )
        vmem = pl.BlockSpec(memory_space=pltpu.VMEM)
        any_ = pl.BlockSpec(memory_space=pl.ANY)
        tgrad, sgrad, wgrad = pl.pallas_call(
            functools.partial(kernel, tuple(scratch), Z, T),
            out_shape=(
                jax.ShapeDtypeStruct((TR // T, D), f32),
                jax.ShapeDtypeStruct((SB, D), f32),
                jax.ShapeDtypeStruct((PART, D), f32),
            ),
            in_specs=[any_, any_, any_, vmem, vmem, any_, any_, any_, any_],
            out_specs=(vmem, vmem, vmem),
            scratch_shapes=list(scratch.values()),
            compiler_params=pltpu.CompilerParams(
                collective_id=0, has_side_effects=True, vmem_limit_bytes=62 * 1024 * 1024
            ),
            name="backward",
        )(target, source, cotangent, target_gain.reshape(1, D), source_gain.reshape(1, D), wq, wk.T, wv.T, wo)
        return tgrad, sgrad, wgrad.T

    return jax.shard_map(
        on_device,
        mesh=mesh,
        in_specs=(
            P("sp", None), P(("sp", "tp"), None), P("sp", None), P(), P(),
            P(None, "tp"), P(None, "tp"), P(None, "tp"), P("tp", None),
        ),
        out_specs=(P(("sp", "tp"), None), P(("sp", "tp"), None), P(None, "tp")),
        check_vma=False,
    )
```

```python
import functools
from types import SimpleNamespace

import jax
import jax.numpy as jnp
from jax import lax
from jax.experimental import pallas as pl
from jax.experimental.pallas import tpu as pltpu
from jax.sharding import PartitionSpec as P

MESH = pl.DeviceIdType.MESH
HEAD = 256
EPSILON = 1e-05
SCALE = HEAD**-0.5
f32 = jnp.float32
bf16 = jnp.bfloat16
SUBS = 8


def nt(left, right):
    return lax.dot_general(left, right, (((1,), (1,)), ((), ())), preferred_element_type=f32)


def nn(left, right):
    return jnp.dot(left, right, preferred_element_type=f32)


def norm(rows):
    centred = rows - jnp.mean(rows, axis=-1, keepdims=True)
    inverse = lax.rsqrt(jnp.mean(centred * centred, axis=-1, keepdims=True) + EPSILON)
    return centred * inverse, inverse


def norm_back(scaled, inverse, gain, upstream):
    weighted = upstream * gain
    spread = jnp.mean(weighted * scaled, axis=-1, keepdims=True)
    return inverse * (weighted - jnp.mean(weighted, axis=-1, keepdims=True) - scaled * spread)


def loop(start, stop, body):
    lax.fori_loop(start, stop, lambda i, carry: (body(i), carry)[1], 0)


def kernel(names, Z, T, *refs):
    (target_h, source_h, cot_h, tgain, sgain, wq_h, wk_h, wv_h, wo_h, tgrad, sgrad, wgrad) = refs[:12]
    s = SimpleNamespace(**dict(zip(names, refs[12:])))
    D = wq_h.shape[0]
    TR = target_h.shape[0]
    SR = T * source_h.shape[0]
    C = T // 2
    HALF = D // 2
    PART = wk_h.shape[0]
    G = HEAD // PART
    z = lax.axis_index("sp")
    t = lax.axis_index("tp")
    c = lax.rem(t, 2)
    p = lax.div(t, 2)
    other = t + 1 - 2 * c
    j = lax.rem(t, G)

    def remote(src, dst, send, recv, **where):
        return pltpu.make_async_remote_copy(
            src_ref=src, dst_ref=dst, send_sem=send, recv_sem=recv, device_id=where, device_id_type=MESH
        )

    def zat(k):
        return lax.rem(z + k + Z, Z)

    def chip(k):
        return lax.rem(p + k, C)

    def same(k):
        return 2 * chip(k) + c

    def mate(k):
        return t - j + lax.rem(j + k, G)

    row0 = pl.multiple_of(p * (TR // C), TR // C)
    loads = [
        pltpu.make_async_copy(a, b, s.in_sem.at[i])
        for i, (a, b) in enumerate(
            (
                (source_h, s.src),
                (target_h, s.tgt),
                (wq_h, s.wq),
                (cot_h, s.cot),
                (wo_h, s.wo),
                (wk_h, s.wkv.at[0:PART, :]),
                (wv_h, s.wkv.at[PART : 2 * PART, :]),
                (target_h.at[pl.ds(row0, TR // C), :], s.t8),
                (cot_h.at[pl.ds(row0, TR // C), :], s.c8),
            )
        )
    ]
    for one in loads:
        one.start()

    barrier = pltpu.get_barrier_semaphore()

    def greet(**where):
        pl.semaphore_signal(barrier, inc=1, device_id=where, device_id_type=MESH)

    loop(1, Z, lambda k: greet(sp=zat(k)))
    loop(1, C, lambda k: greet(tp=same(k)))
    greet(tp=other)
    greet(tp=mate(2) + 1 - 2 * c)

    loads[0].wait()
    scaled, inverse = norm(s.src[...].astype(f32))
    s.src_scaled[...] = scaled
    s.src_inv[...] = jnp.broadcast_to(inverse, s.src_inv.shape)
    s.g[t] = (scaled * sgain[...]).astype(bf16)
    loads[1].wait()

    def norm_target(i):
        rows = pl.ds(pl.multiple_of(i * 32, 32), 32)
        values, _ = norm(s.tgt[rows, :].astype(f32))
        s.tn[rows, :] = (values * tgain[...]).astype(bf16)

    loop(0, TR // 32, norm_target)
    own = pl.ds(pl.multiple_of(z * TR, TR), TR)
    loads[2].wait()
    s.qd[own, 0:HEAD] = nn(s.tn[...], s.wq[...]).astype(bf16)
    loads[3].wait()
    loads[4].wait()
    s.qd[own, HEAD : 2 * HEAD] = nt(s.cot[...], s.wo[...]).astype(bf16)
    pl.semaphore_wait(barrier, (Z - 1) + (C - 1) + 2)

    def source_copy(k):
        return remote(s.g.at[t], s.g.at[t], s.src_send.at[k], s.src_recv.at[t], tp=same(k))

    loop(1, C, lambda k: source_copy(k).start())

    def forward_copy(k):
        row = s.g.at[same(k)]
        return remote(row, row, s.fwd_send.at[k], s.src_recv.at[same(k)], tp=other)

    forward_copy(0).start()
    rows_sub = TR // SUBS

    def ring_copy(block, sub, way, step):
        rows = s.qd.at[pl.ds(pl.multiple_of(block * TR + sub * rows_sub, rows_sub), rows_sub), :]
        return remote(
            rows, rows, s.ring_send.at[way, step, sub], s.ring_recv.at[way, step, sub],
            sp=zat(1 if way == 0 else -1),
        )

    H = Z // 2

    def reach(way, step):
        if step < H:
            return 0, SUBS
        return (0, SUBS // 2) if way == 0 else (SUBS // 2, SUBS)

    for way in (0, 1):
        loop(*reach(way, 1), lambda sub: ring_copy(z, sub, way, 1).start())

    def ring(step, first=-1):
        def arrive(way, sub, on):
            block = zat(-step if way == 0 else step)
            ring_copy(block, sub, way, step).wait_recv()
            if on:
                ring_copy(block, sub, way, step + 1).start()

        def both(lo, hi, on):
            def at(pair):
                for sub in (2 * pair, 2 * pair + 1):
                    arrive(0, sub, on[0])
                    arrive(1, sub, on[1])
                if first >= 0:
                    scores_sent(first + pair)

            loop(lo // 2, hi // 2, at)

        if step < H - 1:
            both(0, SUBS, (True, True))
        elif step == H - 1:
            both(0, SUBS // 2, (True, False))
            both(SUBS // 2, SUBS, (False, True))
        else:

            def last(sub):
                arrive(0, sub, False)
                arrive(1, SUBS // 2 + sub, False)

            loop(first, 2 * H - 1, scores_sent)
            loop(0, SUBS // 2, last)

    loads[5].wait()
    loads[6].wait()

    ring(1)

    def pass_on(k):
        source_copy_from(k).wait_recv()
        forward_copy(k).start()

    def source_copy_from(k):
        row = s.g.at[same(k)]
        return remote(row, row, s.src_send.at[k], s.src_recv.at[same(k)], tp=other)

    loop(1, C, pass_on)
    ring(2)

    def from_other(k):
        at = 2 * chip(k) + 1 - c
        remote(s.g.at[at], s.g.at[at], s.src_send.at[k], s.src_recv.at[at], tp=other).wait_recv()

    ring(3)
    loop(0, C, from_other)

    def stack_rows(q):
        both = jnp.concatenate((s.g[2 * q].astype(f32), s.g[2 * q + 1].astype(f32)), axis=0)
        s.rows[pl.ds(pl.multiple_of(q * 16, 16), 16), :] = both.astype(bf16)

    loop(0, C, stack_rows)
    s.kvp[j] = nt(s.rows[...], s.wkv[...]).astype(bf16)

    def join_copy(k):
        return remote(s.kvp.at[j], s.kvp.at[j], s.join_send.at[k], s.join_recv.at[j], tp=mate(k))

    for k in range(1, G):
        join_copy(k).start()
    ring(4)
    def block_of(k):
        return zat(lax.div(k + 1, 2) * (2 * lax.rem(k, 2) - 1))

    def stat_copy(k):
        b = block_of(k)
        return remote(s.stat.at[b], s.got.at[z], s.stat_send.at[k], s.stat_recv.at[z], sp=lax.rem(b + H, Z))

    def scores(k):
        b = block_of(k)
        rows = pl.ds(pl.multiple_of(b * TR, TR), TR)
        scores_t = nt(s.keys[...], s.qd[rows, 0:HEAD]) * SCALE
        products_t = nt(s.values[...], s.qd[rows, HEAD : 2 * HEAD])
        highest = jnp.max(scores_t, axis=0, keepdims=True)
        weights = jnp.exp(scores_t - highest)
        s.e[b] = weights
        s.p[b] = products_t
        s.stat[b, 0:1, :] = highest
        s.stat[b, 1:2, :] = jnp.sum(weights, axis=0, keepdims=True)
        s.stat[b, 2:3, :] = jnp.sum(weights * products_t, axis=0, keepdims=True)
        s.stat[b, 3:4, :] = highest

    def scores_sent(k):
        scores(k)
        stat_copy(k).start()

    ring(5)
    for k in range(1, G):
        at = lax.rem(j + k, G)
        remote(s.kvp.at[at], s.kvp.at[at], s.join_send.at[k], s.join_recv.at[at], tp=other).wait_recv()
    parts = [s.kvp[i].astype(f32) for i in range(G)]
    keys = jnp.concatenate([a[:, :PART] for a in parts], axis=1)
    s.keys[...] = keys.astype(bf16)
    s.keys_t[...] = keys.T.astype(bf16)
    s.values[...] = jnp.concatenate([a[:, PART:] for a in parts], axis=1).astype(bf16)
    ring(6, 0)
    loop(4, 6, scores_sent)
    ring(7, 6)
    loop(10, 12, scores_sent)
    ring(8, 12)
    scores(15)
    far = zat(H)
    s.got[z] = s.stat[far]

    def stat_wait(k):
        at = block_of(k)
        remote(s.stat.at[at], s.got.at[at], s.stat_send.at[k], s.stat_recv.at[at], sp=at).wait_recv()

    loop(1, Z, stat_wait)
    parts = [s.got[i, 0:1, :] for i in range(Z)]
    top = functools.reduce(jnp.maximum, parts)
    factors = [jnp.exp(a - top) for a in parts]
    total = sum(s.got[i, 1:2, :] * factors[i] for i in range(Z))
    weighted = sum(s.got[i, 2:3, :] * factors[i] for i in range(Z))
    s.fin[far, 0:1, :] = top + jnp.log(total)
    s.fin[far, 1:2, :] = weighted / total

    def fin_copy(k):
        return remote(s.fin.at[far], s.fin.at[far], s.fin_send.at[k], s.fin_recv.at[far], sp=block_of(k))

    loop(1, Z, lambda k: fin_copy(Z - k).start())

    def fin_wait(k):
        at = block_of(k - 1)
        remote(s.fin.at[at], s.fin.at[at], s.fin_send.at[k], s.fin_recv.at[at], sp=at).wait_recv()

    loop(1, Z, fin_wait)

    def slopes(b):
        cols = pl.ds(pl.multiple_of(b * TR, TR), TR)
        weights = s.e[b] * jnp.exp(s.stat[b, 0:1, :] - s.fin[b, 0:1, :])
        s.att[:, cols] = weights.astype(bf16)
        s.slo[:, cols] = (weights * (s.p[b] - s.fin[b, 1:2, :]) * SCALE).astype(bf16)

    for k in range(2 * H - 3, 2 * H):
        b = block_of(k)
        slopes(b)
        cols = pl.ds(pl.multiple_of(b * TR, TR), TR)
        s.dq[:, cols] = nn(s.keys_t[...], s.slo[:, cols])

    hd = HEAD // 2
    STEP = 2

    def sign(way, k):
        return zat(k if way == 1 else -k)

    def hops(way, sub):
        return H if way == sub else H - 1

    def dq_copy(way, k, sub):
        return remote(
            s.dq_out.at[way, k, sub], s.dq_in.at[way, k, sub],
            s.dq_send.at[way, k, sub], s.dq_recv.at[way, k, sub],
            sp=sign(way, k % STEP or STEP),
        )

    def dq_sum(way, k, sub):
        b = sign(way, k) if k else z
        total = s.dq[sub * hd : (sub + 1) * hd, pl.ds(pl.multiple_of(b * TR, TR), TR)]
        if k % STEP == 0:
            for way_in in (way,) if k else (0, 1):
                for far_k in range(k + 1, min(k + STEP, hops(way_in, sub)) + 1):
                    dq_copy(way_in, far_k, sub).wait_recv()
                    total = total + s.dq_in[way_in, far_k, sub].astype(f32)
        return total

    def dq_stage(k):
        for sub in (0, 1):
            for way in (0, 1):
                if k <= hops(way, sub):
                    s.dq_out[way, k, sub] = dq_sum(way, k, sub).astype(bf16)
                    dq_copy(way, k, sub).start()

    dq_stage(8)
    dq_stage(7)
    loop(0, 2 * H - 3, lambda k: slopes(block_of(k)))
    dk = nn(s.slo[...], s.qd[:, 0:HEAD])
    dv = nn(s.att[...], s.qd[:, HEAD : 2 * HEAD])
    for i in range(G):
        cut = slice(i * PART, (i + 1) * PART)
        s.dkv[i] = jnp.concatenate((dk[:, cut], dv[:, cut]), axis=1)
    for k in range(1, G):
        s.dkv_out[k] = s.dkv[lax.rem(j + k, G)].astype(bf16)

    def dkv_copy(k):
        return remote(s.dkv_out.at[k], s.dkv_in.at[k], s.dkv_send.at[k], s.dkv_recv.at[k], tp=mate(k))

    for k in range(1, G):
        dkv_copy(k).start()
    s.dq[...] = nn(s.keys_t[...], s.slo[...])
    dq_stage(6)
    dq_stage(5)
    flat = s.dkv[j]
    for k in range(1, G):
        dkv_copy(k).wait_recv()
        flat = flat + s.dkv_in[k].astype(f32)
    s.flat[...] = flat.astype(bf16)

    part_t = nn(flat.T[:PART, :].astype(bf16), s.rows[...])
    CW = D // Z
    for i in range(Z):
        s.wp[i] = part_t[:, i * CW : (i + 1) * CW].astype(bf16)
    R = H // 2

    def w_copy(way, k):
        hop = k % R or R
        src = s.w_rel.at[way] if k == R else s.wp.at[sign(way, k)]
        return remote(src, s.w_in.at[way, k], s.w_send.at[way, k], s.w_recv.at[way, k], sp=sign(way, hop))

    top_hop = (2 * R, 2 * R - 1)
    for way in (0, 1):
        for k in range(top_hop[way], R, -1):
            w_copy(way, k).start()

    def w_relay():
        for way in (0, 1):
            total = s.wp[sign(way, R)].astype(f32)
            for k in range(R + 1, top_hop[way] + 1):
                w_copy(way, k).wait_recv()
                total = total + s.w_in[way, k].astype(f32)
            s.w_rel[way] = total.astype(bf16)
            w_copy(way, R).start()

    def f_copy(way, k, relay):
        block = sign(1 - way, R) if relay else z
        hop = k - R if relay else k
        return remote(s.wf.at[block], s.wf.at[block], s.f_send.at[way, k], s.f_recv.at[block], sp=sign(way, hop))

    def w_owner():
        total = s.wp[z].astype(f32)
        for way in (0, 1):
            for k in range(1, R + 1):
                w_copy(way, k).wait_recv()
                total = total + s.w_in[way, k].astype(f32)
        s.wf[z] = total.astype(bf16)
        for way in (0, 1):
            for k in range(R, 0, -1):
                f_copy(way, k, False).start()

    def f_wait(k):
        at = block_of(k)
        remote(s.wf.at[at], s.wf.at[at], s.f_send.at[0, k % 2], s.f_recv.at[at], sp=at).wait_recv()

    def f_relay():
        for way in (0, 1):
            f_wait(2 * R - 1 if way == 0 else 2 * R)
            for k in range(top_hop[way], R, -1):
                f_copy(way, k, True).start()

    dq_stage(4)
    dq_stage(3)
    s.su[...] = nn(s.flat[...], s.wkv[...])

    def for_other(q):
        s.ss[q] = s.su[pl.ds(pl.multiple_of(q * 16 + 8 * (1 - c), 8), 8), :].astype(bf16)

    loop(0, C, for_other)
    su_pair = remote(s.ss, s.sr, s.pair_send.at[0], s.pair_recv.at[0], tp=other)
    su_pair.start()
    for way in (0, 1):
        for k in range(R - 1, 0, -1):
            w_copy(way, k).start()
    su_pair.wait_recv()

    def sw_copy(k):
        return remote(s.sv.at[chip(k)], s.sw.at[p], s.sw_send.at[k], s.sw_recv.at[p], tp=same(k))

    def both_cores(k):
        q = chip(k)
        mine = s.su[pl.ds(pl.multiple_of(q * 16 + 8 * c, 8), 8), :]
        return (mine + s.sr[q].astype(f32)).astype(bf16)

    s.sw[p] = both_cores(0)

    def sw_start(k):
        s.sv[chip(k)] = both_cores(k)
        sw_copy(k).start()

    loop(1, C, sw_start)
    w_relay()
    dq_stage(2)
    dq_stage(1)
    w_owner()
    query_flat = jnp.concatenate([dq_sum(0, 0, sub) for sub in (0, 1)], axis=0).T.astype(bf16)

    TB = TR // C

    def half_cols(h):
        return s.wq[pl.ds(pl.multiple_of(h * HALF, HALF), HALF), :]

    s.tsend[...] = nt(query_flat, half_cols(1 - c)).reshape(C, TB, HALF).astype(bf16)
    tu_pair = remote(s.tsend, s.trecv, s.pair_send.at[1], s.pair_recv.at[1], tp=other)
    tu_pair.start()
    s.tmine[...] = nt(query_flat, half_cols(c)).reshape(C, TB, HALF)

    def sw_wait(k):
        at = chip(k)
        remote(s.sv.at[at], s.sw.at[at], s.sw_send.at[k], s.sw_recv.at[at], tp=other).wait_recv()

    tu_pair.wait_recv()

    def tw_copy(k):
        return remote(s.tv.at[chip(k)], s.tw.at[p], s.tw_send.at[k], s.tw_recv.at[p], tp=same(k))

    def tboth(k):
        q = chip(k)
        return (s.tmine[q] + s.trecv[q].astype(f32)).astype(bf16)

    s.tw[p] = tboth(0)

    def tw_start(k):
        s.tv[chip(k)] = tboth(k)
        tw_copy(k).start()

    loop(1, C, tw_start)

    f_relay()
    loop(1, C, sw_wait)
    s.su8[...] = s.sw[0].astype(f32)

    def add_sw(i):
        s.su8[...] += s.sw[i].astype(f32)

    loop(1, C, add_sw)
    sgrad[...] = norm_back(s.src_scaled[...], s.src_inv[:, 0:1], sgain[...], s.su8[...])
    loop(1, C, lambda k: source_copy(k).wait_send())
    loop(0, C, lambda k: forward_copy(k).wait_send())
    for way in (0, 1):
        for step in range(1, H + 1):
            block = zat(-(step - 1) if way == 0 else step - 1)
            loop(*reach(way, step), lambda sub: ring_copy(block, sub, way, step).wait_send())
    for k in range(1, G):
        join_copy(k).wait_send()
        dkv_copy(k).wait_send()

    def line_sends(k):
        stat_copy(k - 1).wait_send()
        fin_copy(k).wait_send()

    loop(1, Z, line_sends)
    for way in (0, 1):
        for sub in (0, 1):
            for k in range(1, hops(way, sub) + 1):
                dq_copy(way, k, sub).wait_send()
        for k in range(1, top_hop[way] + 1):
            w_copy(way, k).wait_send()
    su_pair.wait_send()
    loop(1, C, lambda k: sw_copy(k).wait_send())

    def tw_wait(k):
        at = chip(k)
        remote(s.tv.at[at], s.tw.at[at], s.tw_send.at[k], s.tw_recv.at[at], tp=other).wait_recv()

    loop(1, C, tw_wait)
    s.tu8[...] = s.tw[0].astype(f32)

    def add_tw(i):
        s.tu8[...] += s.tw[i].astype(f32)

    loop(1, C, add_tw)
    TO = TB // 2
    lower, upper = s.tu8[0:TO, :], s.tu8[TO:TB, :]
    mine = jnp.where(c == 0, lower, upper)
    s.tx_out[...] = jnp.where(c == 0, upper, lower)
    last_pair = remote(s.tx_out, s.tx_in, s.pair_send.at[2], s.pair_recv.at[2], tp=other)
    last_pair.start()
    loads[7].wait()
    loads[8].wait()
    scaled, inverse = norm(s.t8[...].astype(f32))
    cot = s.c8[...].astype(f32)
    scaled = jnp.where(c == 0, scaled[0:TO], scaled[TO:TB])
    inverse = jnp.where(c == 0, inverse[0:TO], inverse[TO:TB])
    cot = jnp.where(c == 0, cot[0:TO], cot[TO:TB])
    last_pair.wait_recv()
    theirs = s.tx_in[...]
    upstream = jnp.concatenate(
        (jnp.where(c == 0, mine, theirs), jnp.where(c == 0, theirs, mine)), axis=1
    )
    tgrad[...] = cot + norm_back(scaled, inverse, tgain[...], upstream)

    for k in range(1, Z):
        if k not in (2 * R - 1, 2 * R):
            f_wait(k)
    for i in range(Z):
        wgrad[:, i * CW : (i + 1) * CW] = s.wf[i]
    for way in (0, 1):
        for k in range(1, top_hop[way] + 1):
            f_copy(way, k, k > R).wait_send()
    loop(1, C, lambda k: tw_copy(k).wait_send())
    tu_pair.wait_send()
    last_pair.wait_send()


def put(tgrad, sgrad, wgrad, tgrad_out, sgrad_out, wgrad_out):
    tgrad_out[...] = tgrad[...]
    sgrad_out[...] = sgrad[...]
    wgrad_out[...] = wgrad[...].astype(f32)


def solution(mesh):
    Z, T = mesh.shape["sp"], mesh.shape["tp"]

    def on_device(target, source, cotangent, target_gain, source_gain, wq, wk, wv, wo):
        TR, D = target.shape
        SB = source.shape[0]
        SR = SB * T
        C = T // 2
        PART = wk.shape[1]
        G = HEAD // PART
        H = Z // 2
        TB = TR // C
        CW = D // Z
        V = pltpu.VMEM
        dma = pltpu.SemaphoreType.DMA
        scratch = dict(
            src=V((SB, D), bf16), tgt=V((TR, D), bf16), cot=V((TR, D), bf16),
            wq=V((D, HEAD), bf16), wo=V((HEAD, D), bf16),
            t8=V((TB, D), bf16), c8=V((TB, D), bf16),
            src_scaled=V((SB, D), f32), src_inv=V((SB, 128), f32),
            g=V((T, SB, D), bf16), tn=V((TR, D), bf16), qd=V((Z * TR, 2 * HEAD), bf16),
            wkv=V((2 * PART, D), bf16), rows=V((SR, D), bf16), kvp=V((G, SR, 2 * PART), bf16),
            keys=V((SR, HEAD), bf16), keys_t=V((HEAD, SR), bf16), values=V((SR, HEAD), bf16),
            e=V((Z, SR, TR), f32), p=V((Z, SR, TR), f32),
            stat=V((Z, 4, TR), f32), got=V((Z, 4, TR), f32), fin=V((Z, 2, TR), f32),
            att=V((SR, Z * TR), bf16), slo=V((SR, Z * TR), bf16), dq=V((HEAD, Z * TR), f32),
            dq_out=V((2, H + 1, 2, HEAD // 2, TR), bf16), dq_in=V((2, H + 1, 2, HEAD // 2, TR), bf16),
            dkv=V((G, SR, 2 * PART), f32), dkv_out=V((G, SR, 2 * PART), bf16), dkv_in=V((G, SR, 2 * PART), bf16),
            flat=V((SR, 2 * PART), bf16),
            wp=V((Z, PART, CW), bf16), w_in=V((2, H + 1, PART, CW), bf16), w_rel=V((2, PART, CW), bf16),
            wf=V((Z, PART, CW), bf16),
            su=V((SR, D), f32), ss=V((C, SB, D), bf16), sr=V((C, SB, D), bf16),
            sv=V((C, SB, D), bf16), sw=V((C, SB, D), bf16), su8=V((SB, D), f32),
            tsend=V((C, TB, D // 2), bf16), trecv=V((C, TB, D // 2), bf16), tmine=V((C, TB, D // 2), f32),
            tv=V((C, TB, D // 2), bf16), tw=V((C, TB, D // 2), bf16), tu8=V((TB, D // 2), f32),
            tx_out=V((TB // 2, D // 2), f32), tx_in=V((TB // 2, D // 2), f32),
            in_sem=dma((9,)), src_send=dma((C,)), fwd_send=dma((C,)), src_recv=dma((T,)),
            ring_send=dma((2, H + 1, SUBS)), ring_recv=dma((2, H + 1, SUBS)),
            join_send=dma((G,)), join_recv=dma((G,)), dkv_send=dma((G,)), dkv_recv=dma((G,)),
            stat_send=dma((Z,)), stat_recv=dma((Z,)), fin_send=dma((Z,)), fin_recv=dma((Z,)),
            w_send=dma((2, H + 1)), w_recv=dma((2, H + 1)), f_send=dma((2, H + 1)), f_recv=dma((Z,)),
            dq_send=dma((2, H + 1, 2)), dq_recv=dma((2, H + 1, 2)),
            sw_send=dma((C,)), sw_recv=dma((C,)), tw_send=dma((C,)), tw_recv=dma((C,)),
            pair_send=dma((3,)), pair_recv=dma((3,)),
        )
        vmem = pl.BlockSpec(memory_space=pltpu.VMEM)
        any_ = pl.BlockSpec(memory_space=pl.ANY)
        tgrad, sgrad, wgrad = pl.pallas_call(
            functools.partial(kernel, tuple(scratch), Z, T),
            out_shape=(
                jax.ShapeDtypeStruct((TR // T, D), f32),
                jax.ShapeDtypeStruct((SB, D), f32),
                jax.ShapeDtypeStruct((PART, D), bf16),
            ),
            in_specs=[any_, any_, any_, vmem, vmem, any_, any_, any_, any_],
            out_specs=(vmem, vmem, vmem),
            scratch_shapes=list(scratch.values()),
            compiler_params=pltpu.CompilerParams(
                collective_id=0, has_side_effects=True, vmem_limit_bytes=62 * 1024 * 1024
            ),
            name="backward",
        )(target, source, cotangent, target_gain.reshape(1, D), source_gain.reshape(1, D), wq, wk.T, wv.T, wo)
        tgrad, sgrad, wgrad = pl.pallas_call(
            put,
            out_shape=(
                jax.ShapeDtypeStruct((TR // T, D), f32),
                jax.ShapeDtypeStruct((SB, D), f32),
                jax.ShapeDtypeStruct((PART, D), f32),
            ),
            in_specs=[vmem, vmem, vmem],
            out_specs=(vmem, vmem, vmem),
            name="put",
        )(tgrad, sgrad, wgrad)
        return tgrad, sgrad, wgrad.T

    return jax.shard_map(
        on_device,
        mesh=mesh,
        in_specs=(
            P("sp", None), P(("sp", "tp"), None), P("sp", None), P(), P(),
            P(None, "tp"), P(None, "tp"), P(None, "tp"), P("tp", None),
        ),
        out_specs=(P(("sp", "tp"), None), P(("sp", "tp"), None), P(None, "tp")),
        check_vma=False,
    )
```

```python
import functools
from types import SimpleNamespace

import jax
import jax.numpy as jnp
from jax import lax
from jax.experimental import pallas as pl
from jax.experimental.pallas import tpu as pltpu
from jax.sharding import PartitionSpec as P

MESH = pl.DeviceIdType.MESH
HEAD = 256
EPSILON = 1e-05
SCALE = HEAD**-0.5
f32 = jnp.float32
bf16 = jnp.bfloat16
SUBS = 8


def nt(left, right):
    return lax.dot_general(left, right, (((1,), (1,)), ((), ())), preferred_element_type=f32)


def nn(left, right):
    return jnp.dot(left, right, preferred_element_type=f32)


def norm(rows):
    centred = rows - jnp.mean(rows, axis=-1, keepdims=True)
    inverse = lax.rsqrt(jnp.mean(centred * centred, axis=-1, keepdims=True) + EPSILON)
    return centred * inverse, inverse


def norm_back(scaled, inverse, gain, upstream):
    weighted = upstream * gain
    spread = jnp.mean(weighted * scaled, axis=-1, keepdims=True)
    return inverse * (weighted - jnp.mean(weighted, axis=-1, keepdims=True) - scaled * spread)


def loop(start, stop, body):
    lax.fori_loop(start, stop, lambda i, carry: (body(i), carry)[1], 0)


def kernel(names, Z, T, *refs):
    (target_h, source_h, cot_h, tgain, sgain, wq_h, wk_h, wv_h, wo_h, tgrad, sgrad, wgrad) = refs[:12]
    s = SimpleNamespace(**dict(zip(names, refs[12:])))
    D = wq_h.shape[0]
    TR = target_h.shape[0]
    SR = T * source_h.shape[0]
    C = T // 2
    HALF = D // 2
    PART = wk_h.shape[0]
    G = HEAD // PART
    z = lax.axis_index("sp")
    t = lax.axis_index("tp")
    c = lax.rem(t, 2)
    p = lax.div(t, 2)
    other = t + 1 - 2 * c
    j = lax.rem(t, G)

    def remote(src, dst, send, recv, **where):
        return pltpu.make_async_remote_copy(
            src_ref=src, dst_ref=dst, send_sem=send, recv_sem=recv, device_id=where, device_id_type=MESH
        )

    def zat(k):
        return lax.rem(z + k + Z, Z)

    def chip(k):
        return lax.rem(p + k, C)

    def same(k):
        return 2 * chip(k) + c

    def mate(k):
        return t - j + lax.rem(j + k, G)

    row0 = pl.multiple_of(p * (TR // C), TR // C)
    loads = [
        pltpu.make_async_copy(a, b, s.in_sem.at[i])
        for i, (a, b) in enumerate(
            (
                (source_h, s.src),
                (target_h, s.tgt),
                (wq_h, s.wq),
                (cot_h, s.cot),
                (wo_h, s.wo),
                (wk_h, s.wkv.at[0:PART, :]),
                (wv_h, s.wkv.at[PART : 2 * PART, :]),
                (target_h.at[pl.ds(row0, TR // C), :], s.t8),
                (cot_h.at[pl.ds(row0, TR // C), :], s.c8),
            )
        )
    ]
    for one in loads:
        one.start()

    barrier = pltpu.get_barrier_semaphore()

    def greet(**where):
        pl.semaphore_signal(barrier, inc=1, device_id=where, device_id_type=MESH)

    loop(1, Z, lambda k: greet(sp=zat(k)))
    loop(1, C, lambda k: greet(tp=same(k)))
    greet(tp=other)
    greet(tp=mate(2) + 1 - 2 * c)

    loads[0].wait()
    scaled, inverse = norm(s.src[...].astype(f32))
    s.src_scaled[...] = scaled
    s.src_inv[...] = jnp.broadcast_to(inverse, s.src_inv.shape)
    s.g[t] = (scaled * sgain[...]).astype(bf16)
    loads[1].wait()

    def norm_target(i):
        rows = pl.ds(pl.multiple_of(i * 32, 32), 32)
        values, _ = norm(s.tgt[rows, :].astype(f32))
        s.tn[rows, :] = (values * tgain[...]).astype(bf16)

    loop(0, TR // 32, norm_target)
    own = pl.ds(pl.multiple_of(z * TR, TR), TR)
    loads[2].wait()
    s.qd[own, 0:HEAD] = nn(s.tn[...], s.wq[...]).astype(bf16)
    loads[3].wait()
    loads[4].wait()
    s.qd[own, HEAD : 2 * HEAD] = nt(s.cot[...], s.wo[...]).astype(bf16)
    pl.semaphore_wait(barrier, (Z - 1) + (C - 1) + 2)

    def source_copy(k):
        return remote(s.g.at[t], s.g.at[t], s.src_send.at[k], s.src_recv.at[t], tp=same(k))

    loop(1, C, lambda k: source_copy(k).start())

    def forward_copy(k):
        row = s.g.at[same(k)]
        return remote(row, row, s.fwd_send.at[k], s.src_recv.at[same(k)], tp=other)

    forward_copy(0).start()
    rows_sub = TR // SUBS

    def ring_copy(block, sub, way, step):
        rows = s.qd.at[pl.ds(pl.multiple_of(block * TR + sub * rows_sub, rows_sub), rows_sub), :]
        return remote(
            rows, rows, s.ring_send.at[way, step, sub], s.ring_recv.at[way, step, sub],
            sp=zat(1 if way == 0 else -1),
        )

    H = Z // 2

    def reach(way, step):
        if step < H:
            return 0, SUBS
        return (0, SUBS // 2) if way == 0 else (SUBS // 2, SUBS)

    for way in (0, 1):
        loop(*reach(way, 1), lambda sub: ring_copy(z, sub, way, 1).start())

    def ring(step, first=-1):
        def arrive(way, sub, on):
            block = zat(-step if way == 0 else step)
            ring_copy(block, sub, way, step).wait_recv()
            if on:
                ring_copy(block, sub, way, step + 1).start()

        def both(lo, hi, on):
            def at(pair):
                for sub in (2 * pair, 2 * pair + 1):
                    arrive(0, sub, on[0])
                    arrive(1, sub, on[1])
                if first >= 0:
                    scores_sent(first + pair)

            loop(lo // 2, hi // 2, at)

        if step < H - 1:
            both(0, SUBS, (True, True))
        elif step == H - 1:
            both(0, SUBS // 2, (True, False))
            both(SUBS // 2, SUBS, (False, True))
        else:

            def last(sub):
                arrive(0, sub, False)
                arrive(1, SUBS // 2 + sub, False)

            loop(first, 2 * H - 1, scores_sent)
            loop(0, SUBS // 2, last)

    loads[5].wait()
    loads[6].wait()

    ring(1)

    def pass_on(k):
        source_copy_from(k).wait_recv()
        forward_copy(k).start()

    def source_copy_from(k):
        row = s.g.at[same(k)]
        return remote(row, row, s.src_send.at[k], s.src_recv.at[same(k)], tp=other)

    loop(1, C // 2, pass_on)
    ring(2)
    loop(C // 2, C, pass_on)

    def from_other(k):
        at = 2 * chip(k) + 1 - c
        remote(s.g.at[at], s.g.at[at], s.src_send.at[k], s.src_recv.at[at], tp=other).wait_recv()

    ring(3)
    loop(0, C, from_other)

    def stack_rows(q):
        both = jnp.concatenate((s.g[2 * q].astype(f32), s.g[2 * q + 1].astype(f32)), axis=0)
        s.rows[pl.ds(pl.multiple_of(q * 16, 16), 16), :] = both.astype(bf16)

    loop(0, C, stack_rows)
    s.kvp[j] = nt(s.rows[...], s.wkv[...]).astype(bf16)

    def join_copy(k):
        return remote(s.kvp.at[j], s.kvp.at[j], s.join_send.at[k], s.join_recv.at[j], tp=mate(k))

    for k in range(1, G):
        join_copy(k).start()
    ring(4)
    def block_of(k):
        return zat(lax.div(k + 1, 2) * (2 * lax.rem(k, 2) - 1))

    def stat_copy(k):
        b = block_of(k)
        return remote(s.stat.at[b], s.got.at[z], s.stat_send.at[k], s.stat_recv.at[z], sp=lax.rem(b + H, Z))

    def scores(k):
        b = block_of(k)
        rows = pl.ds(pl.multiple_of(b * TR, TR), TR)
        scores_t = nt(s.keys[...], s.qd[rows, 0:HEAD]) * SCALE
        products_t = nt(s.values[...], s.qd[rows, HEAD : 2 * HEAD])
        highest = jnp.max(scores_t, axis=0, keepdims=True)
        weights = jnp.exp(scores_t - highest)
        s.e[b] = weights
        s.p[b] = products_t
        s.stat[b, 0:1, :] = highest
        s.stat[b, 1:2, :] = jnp.sum(weights, axis=0, keepdims=True)
        s.stat[b, 2:3, :] = jnp.sum(weights * products_t, axis=0, keepdims=True)
        s.stat[b, 3:4, :] = highest

    def scores_sent(k):
        scores(k)
        stat_copy(k).start()

    ring(5)
    for k in range(1, G):
        at = lax.rem(j + k, G)
        remote(s.kvp.at[at], s.kvp.at[at], s.join_send.at[k], s.join_recv.at[at], tp=other).wait_recv()
    parts = [s.kvp[i].astype(f32) for i in range(G)]
    keys = jnp.concatenate([a[:, :PART] for a in parts], axis=1)
    s.keys[...] = keys.astype(bf16)
    s.keys_t[...] = keys.T.astype(bf16)
    s.values[...] = jnp.concatenate([a[:, PART:] for a in parts], axis=1).astype(bf16)
    ring(6, 0)
    loop(4, 6, scores_sent)
    ring(7, 6)
    loop(10, 12, scores_sent)
    ring(8, 12)
    scores(15)
    far = zat(H)
    s.got[z] = s.stat[far]

    def stat_wait(k):
        at = block_of(k)
        remote(s.stat.at[at], s.got.at[at], s.stat_send.at[k], s.stat_recv.at[at], sp=at).wait_recv()

    loop(1, Z, stat_wait)
    parts = [s.got[i, 0:1, :] for i in range(Z)]
    top = functools.reduce(jnp.maximum, parts)
    factors = [jnp.exp(a - top) for a in parts]
    total = sum(s.got[i, 1:2, :] * factors[i] for i in range(Z))
    weighted = sum(s.got[i, 2:3, :] * factors[i] for i in range(Z))
    s.fin[far, 0:1, :] = top + jnp.log(total)
    s.fin[far, 1:2, :] = weighted / total

    def fin_copy(k):
        return remote(s.fin.at[far], s.fin.at[far], s.fin_send.at[k], s.fin_recv.at[far], sp=block_of(k))

    loop(1, Z, lambda k: fin_copy(Z - k).start())

    def fin_wait(k):
        at = block_of(k)
        remote(s.fin.at[at], s.fin.at[at], s.fin_send.at[k], s.fin_recv.at[at], sp=at).wait_recv()

    def slopes(b):
        cols = pl.ds(pl.multiple_of(b * TR, TR), TR)
        weights = s.e[b] * jnp.exp(s.stat[b, 0:1, :] - s.fin[b, 0:1, :])
        s.att[:, cols] = weights.astype(bf16)
        s.slo[:, cols] = (weights * (s.p[b] - s.fin[b, 1:2, :]) * SCALE).astype(bf16)

    hd = HEAD // 2
    STEP = 2

    def sign(way, k):
        return zat(k if way == 1 else -k)

    def hops(way, sub):
        return H if way == sub else H - 1

    def dq_copy(way, k, sub):
        return remote(
            s.dq_out.at[way, k, sub], s.dq_in.at[way, k, sub],
            s.dq_send.at[way, k, sub], s.dq_recv.at[way, k, sub],
            sp=sign(way, k % STEP or STEP),
        )

    def dq_sum(way, k, sub):
        b = sign(way, k) if k else z
        total = s.dq[sub * hd : (sub + 1) * hd, pl.ds(pl.multiple_of(b * TR, TR), TR)]
        if k % STEP == 0:
            for way_in in (way,) if k else (0, 1):
                for far_k in range(k + 1, min(k + STEP, hops(way_in, sub)) + 1):
                    dq_copy(way_in, far_k, sub).wait_recv()
                    total = total + s.dq_in[way_in, far_k, sub].astype(f32)
        return total

    def dq_stage(k):
        for sub in (0, 1):
            for way in (0, 1):
                if k <= hops(way, sub):
                    s.dq_out[way, k, sub] = dq_sum(way, k, sub).astype(bf16)
                    dq_copy(way, k, sub).start()

    def settle(k):
        fin_wait(k)
        slopes(block_of(k))

    def part(k):
        cols = pl.ds(pl.multiple_of(block_of(k) * TR, TR), TR)
        s.dq[:, cols] = nn(s.keys_t[...], s.slo[:, cols])

    slopes(far)
    part(2 * H - 1)
    dq_stage(8)
    for k in (13, 14):
        settle(k)
        part(k)
    dq_stage(7)
    for k in (11, 12, 9, 10):
        settle(k)
        part(k)
    dq_stage(5)
    loop(0, 4, lambda i: settle(8 - i))
    dq_stage(6)
    loop(0, 5, lambda i: settle(4 - i))
    dk = nn(s.slo[...], s.qd[:, 0:HEAD])
    dv = nn(s.att[...], s.qd[:, HEAD : 2 * HEAD])
    for i in range(G):
        cut = slice(i * PART, (i + 1) * PART)
        s.dkv[i] = jnp.concatenate((dk[:, cut], dv[:, cut]), axis=1)
    for k in range(1, G):
        s.dkv_out[k] = s.dkv[lax.rem(j + k, G)].astype(bf16)

    def dkv_copy(k):
        return remote(s.dkv_out.at[k], s.dkv_in.at[k], s.dkv_send.at[k], s.dkv_recv.at[k], tp=mate(k))

    for k in range(1, G):
        dkv_copy(k).start()
    s.dq[...] = nn(s.keys_t[...], s.slo[...])
    dq_stage(3)
    dq_stage(4)
    flat = s.dkv[j]
    for k in range(1, G):
        dkv_copy(k).wait_recv()
        flat = flat + s.dkv_in[k].astype(f32)
    s.flat[...] = flat.astype(bf16)

    part_t = nn(flat.T[:PART, :].astype(bf16), s.rows[...])
    CW = D // Z
    for i in range(Z):
        s.wp[i] = part_t[:, i * CW : (i + 1) * CW].astype(bf16)
    R = H // 2

    def w_copy(way, k):
        hop = k % R or R
        src = s.w_rel.at[way] if k == R else s.wp.at[sign(way, k)]
        return remote(src, s.w_in.at[way, k], s.w_send.at[way, k], s.w_recv.at[way, k], sp=sign(way, hop))

    top_hop = (2 * R, 2 * R - 1)
    for way in (0, 1):
        for k in range(top_hop[way], R, -1):
            w_copy(way, k).start()

    def w_relay():
        for way in (0, 1):
            total = s.wp[sign(way, R)].astype(f32)
            for k in range(R + 1, top_hop[way] + 1):
                w_copy(way, k).wait_recv()
                total = total + s.w_in[way, k].astype(f32)
            s.w_rel[way] = total.astype(bf16)
            w_copy(way, R).start()

    def f_copy(way, k, relay):
        block = sign(1 - way, R) if relay else z
        hop = k - R if relay else k
        return remote(s.wf.at[block], s.wf.at[block], s.f_send.at[way, k], s.f_recv.at[block], sp=sign(way, hop))

    def w_owner():
        total = s.wp[z].astype(f32)
        for way in (0, 1):
            for k in range(1, R + 1):
                w_copy(way, k).wait_recv()
                total = total + s.w_in[way, k].astype(f32)
        s.wf[z] = total.astype(bf16)
        for way in (0, 1):
            for k in range(R, 0, -1):
                f_copy(way, k, False).start()

    def f_wait(k):
        at = block_of(k)
        remote(s.wf.at[at], s.wf.at[at], s.f_send.at[0, k % 2], s.f_recv.at[at], sp=at).wait_recv()

    def f_relay():
        for way in (0, 1):
            f_wait(2 * R - 1 if way == 0 else 2 * R)
            for k in range(top_hop[way], R, -1):
                f_copy(way, k, True).start()

    dq_stage(1)
    s.su[...] = nn(s.flat[...], s.wkv[...])

    def for_other(q):
        s.ss[q] = s.su[pl.ds(pl.multiple_of(q * 16 + 8 * (1 - c), 8), 8), :].astype(bf16)

    loop(0, C, for_other)
    su_pair = remote(s.ss, s.sr, s.pair_send.at[0], s.pair_recv.at[0], tp=other)
    su_pair.start()
    for way in (0, 1):
        for k in range(R - 1, 0, -1):
            w_copy(way, k).start()
    dq_stage(2)
    su_pair.wait_recv()

    def sw_copy(k):
        return remote(s.sv.at[chip(k)], s.sw.at[p], s.sw_send.at[k], s.sw_recv.at[p], tp=same(k))

    def both_cores(k):
        q = chip(k)
        mine = s.su[pl.ds(pl.multiple_of(q * 16 + 8 * c, 8), 8), :]
        return (mine + s.sr[q].astype(f32)).astype(bf16)

    s.sw[p] = both_cores(0)

    def sw_start(k):
        s.sv[chip(k)] = both_cores(k)
        sw_copy(k).start()

    loop(1, C, sw_start)
    w_relay()
    query_flat = jnp.concatenate([dq_sum(0, 0, sub) for sub in (0, 1)], axis=0).T.astype(bf16)

    TB = TR // C

    def half_cols(h):
        return s.wq[pl.ds(pl.multiple_of(h * HALF, HALF), HALF), :]

    s.tsend[...] = nt(query_flat, half_cols(1 - c)).reshape(C, TB, HALF).astype(bf16)
    tu_pair = remote(s.tsend, s.trecv, s.pair_send.at[1], s.pair_recv.at[1], tp=other)
    tu_pair.start()
    s.tmine[...] = nt(query_flat, half_cols(c)).reshape(C, TB, HALF)

    def sw_wait(k):
        at = chip(k)
        remote(s.sv.at[at], s.sw.at[at], s.sw_send.at[k], s.sw_recv.at[at], tp=other).wait_recv()

    w_owner()
    tu_pair.wait_recv()

    def tw_copy(k):
        return remote(s.tv.at[chip(k)], s.tw.at[p], s.tw_send.at[k], s.tw_recv.at[p], tp=same(k))

    def tboth(k):
        q = chip(k)
        return (s.tmine[q] + s.trecv[q].astype(f32)).astype(bf16)

    s.tw[p] = tboth(0)

    def tw_start(k):
        s.tv[chip(k)] = tboth(k)
        tw_copy(k).start()

    loop(1, C, tw_start)

    loop(1, C, sw_wait)
    s.su8[...] = s.sw[0].astype(f32)

    def add_sw(i):
        s.su8[...] += s.sw[i].astype(f32)

    loop(1, C, add_sw)
    sgrad[...] = norm_back(s.src_scaled[...], s.src_inv[:, 0:1], sgain[...], s.su8[...])
    f_relay()
    loop(1, C, lambda k: source_copy(k).wait_send())
    loop(0, C, lambda k: forward_copy(k).wait_send())
    for way in (0, 1):
        for step in range(1, H + 1):
            block = zat(-(step - 1) if way == 0 else step - 1)
            loop(*reach(way, step), lambda sub: ring_copy(block, sub, way, step).wait_send())
    for k in range(1, G):
        join_copy(k).wait_send()
        dkv_copy(k).wait_send()

    def line_sends(k):
        stat_copy(k - 1).wait_send()
        fin_copy(k).wait_send()

    loop(1, Z, line_sends)
    for way in (0, 1):
        for sub in (0, 1):
            for k in range(1, hops(way, sub) + 1):
                dq_copy(way, k, sub).wait_send()
        for k in range(1, top_hop[way] + 1):
            w_copy(way, k).wait_send()
    su_pair.wait_send()
    loop(1, C, lambda k: sw_copy(k).wait_send())

    def tw_wait(k):
        at = chip(k)
        remote(s.tv.at[at], s.tw.at[at], s.tw_send.at[k], s.tw_recv.at[at], tp=other).wait_recv()

    loop(1, C, tw_wait)
    s.tu8[...] = s.tw[0].astype(f32)

    def add_tw(i):
        s.tu8[...] += s.tw[i].astype(f32)

    loop(1, C, add_tw)
    TO = TB // 2
    lower, upper = s.tu8[0:TO, :], s.tu8[TO:TB, :]
    mine = jnp.where(c == 0, lower, upper)
    s.tx_out[...] = jnp.where(c == 0, upper, lower)
    last_pair = remote(s.tx_out, s.tx_in, s.pair_send.at[2], s.pair_recv.at[2], tp=other)
    last_pair.start()
    loads[7].wait()
    loads[8].wait()
    scaled, inverse = norm(s.t8[...].astype(f32))
    cot = s.c8[...].astype(f32)
    scaled = jnp.where(c == 0, scaled[0:TO], scaled[TO:TB])
    inverse = jnp.where(c == 0, inverse[0:TO], inverse[TO:TB])
    cot = jnp.where(c == 0, cot[0:TO], cot[TO:TB])
    last_pair.wait_recv()
    theirs = s.tx_in[...]
    upstream = jnp.concatenate(
        (jnp.where(c == 0, mine, theirs), jnp.where(c == 0, theirs, mine)), axis=1
    )
    tgrad[...] = cot + norm_back(scaled, inverse, tgain[...], upstream)

    for k in range(1, Z):
        if k not in (2 * R - 1, 2 * R):
            f_wait(k)
    for i in range(Z):
        wgrad[:, i * CW : (i + 1) * CW] = s.wf[i]
    for way in (0, 1):
        for k in range(1, top_hop[way] + 1):
            f_copy(way, k, k > R).wait_send()
    loop(1, C, lambda k: tw_copy(k).wait_send())
    tu_pair.wait_send()
    last_pair.wait_send()


def put(tgrad, sgrad, wgrad, tgrad_out, sgrad_out, wgrad_out):
    tgrad_out[...] = tgrad[...]
    sgrad_out[...] = sgrad[...]
    wgrad_out[...] = wgrad[...].astype(f32)


def solution(mesh):
    Z, T = mesh.shape["sp"], mesh.shape["tp"]

    def on_device(target, source, cotangent, target_gain, source_gain, wq, wk, wv, wo):
        TR, D = target.shape
        SB = source.shape[0]
        SR = SB * T
        C = T // 2
        PART = wk.shape[1]
        G = HEAD // PART
        H = Z // 2
        TB = TR // C
        CW = D // Z
        V = pltpu.VMEM
        dma = pltpu.SemaphoreType.DMA
        scratch = dict(
            src=V((SB, D), bf16), tgt=V((TR, D), bf16), cot=V((TR, D), bf16),
            wq=V((D, HEAD), bf16), wo=V((HEAD, D), bf16),
            t8=V((TB, D), bf16), c8=V((TB, D), bf16),
            src_scaled=V((SB, D), f32), src_inv=V((SB, 128), f32),
            g=V((T, SB, D), bf16), tn=V((TR, D), bf16), qd=V((Z * TR, 2 * HEAD), bf16),
            wkv=V((2 * PART, D), bf16), rows=V((SR, D), bf16), kvp=V((G, SR, 2 * PART), bf16),
            keys=V((SR, HEAD), bf16), keys_t=V((HEAD, SR), bf16), values=V((SR, HEAD), bf16),
            e=V((Z, SR, TR), f32), p=V((Z, SR, TR), f32),
            stat=V((Z, 4, TR), f32), got=V((Z, 4, TR), f32), fin=V((Z, 2, TR), f32),
            att=V((SR, Z * TR), bf16), slo=V((SR, Z * TR), bf16), dq=V((HEAD, Z * TR), f32),
            dq_out=V((2, H + 1, 2, HEAD // 2, TR), bf16), dq_in=V((2, H + 1, 2, HEAD // 2, TR), bf16),
            dkv=V((G, SR, 2 * PART), f32), dkv_out=V((G, SR, 2 * PART), bf16), dkv_in=V((G, SR, 2 * PART), bf16),
            flat=V((SR, 2 * PART), bf16),
            wp=V((Z, PART, CW), bf16), w_in=V((2, H + 1, PART, CW), bf16), w_rel=V((2, PART, CW), bf16),
            wf=V((Z, PART, CW), bf16),
            su=V((SR, D), f32), ss=V((C, SB, D), bf16), sr=V((C, SB, D), bf16),
            sv=V((C, SB, D), bf16), sw=V((C, SB, D), bf16), su8=V((SB, D), f32),
            tsend=V((C, TB, D // 2), bf16), trecv=V((C, TB, D // 2), bf16), tmine=V((C, TB, D // 2), f32),
            tv=V((C, TB, D // 2), bf16), tw=V((C, TB, D // 2), bf16), tu8=V((TB, D // 2), f32),
            tx_out=V((TB // 2, D // 2), f32), tx_in=V((TB // 2, D // 2), f32),
            in_sem=dma((9,)), src_send=dma((C,)), fwd_send=dma((C,)), src_recv=dma((T,)),
            ring_send=dma((2, H + 1, SUBS)), ring_recv=dma((2, H + 1, SUBS)),
            join_send=dma((G,)), join_recv=dma((G,)), dkv_send=dma((G,)), dkv_recv=dma((G,)),
            stat_send=dma((Z,)), stat_recv=dma((Z,)), fin_send=dma((Z,)), fin_recv=dma((Z,)),
            w_send=dma((2, H + 1)), w_recv=dma((2, H + 1)), f_send=dma((2, H + 1)), f_recv=dma((Z,)),
            dq_send=dma((2, H + 1, 2)), dq_recv=dma((2, H + 1, 2)),
            sw_send=dma((C,)), sw_recv=dma((C,)), tw_send=dma((C,)), tw_recv=dma((C,)),
            pair_send=dma((3,)), pair_recv=dma((3,)),
        )
        vmem = pl.BlockSpec(memory_space=pltpu.VMEM)
        any_ = pl.BlockSpec(memory_space=pl.ANY)
        tgrad, sgrad, wgrad = pl.pallas_call(
            functools.partial(kernel, tuple(scratch), Z, T),
            out_shape=(
                jax.ShapeDtypeStruct((TR // T, D), f32),
                jax.ShapeDtypeStruct((SB, D), f32),
                jax.ShapeDtypeStruct((PART, D), bf16),
            ),
            in_specs=[any_, any_, any_, vmem, vmem, any_, any_, any_, any_],
            out_specs=(vmem, vmem, vmem),
            scratch_shapes=list(scratch.values()),
            compiler_params=pltpu.CompilerParams(
                collective_id=0, has_side_effects=True, vmem_limit_bytes=62 * 1024 * 1024
            ),
            name="backward",
        )(target, source, cotangent, target_gain.reshape(1, D), source_gain.reshape(1, D), wq, wk.T, wv.T, wo)
        tgrad, sgrad, wgrad = pl.pallas_call(
            put,
            out_shape=(
                jax.ShapeDtypeStruct((TR // T, D), f32),
                jax.ShapeDtypeStruct((SB, D), f32),
                jax.ShapeDtypeStruct((PART, D), f32),
            ),
            in_specs=[vmem, vmem, vmem],
            out_specs=(vmem, vmem, vmem),
            name="put",
        )(tgrad, sgrad, wgrad)
        return tgrad, sgrad, wgrad.T

    return jax.shard_map(
        on_device,
        mesh=mesh,
        in_specs=(
            P("sp", None), P(("sp", "tp"), None), P("sp", None), P(), P(),
            P(None, "tp"), P(None, "tp"), P(None, "tp"), P("tp", None),
        ),
        out_specs=(P(("sp", "tp"), None), P(("sp", "tp"), None), P(None, "tp")),
        check_vma=False,
    )
```

```python
import functools
from types import SimpleNamespace

import jax
import jax.numpy as jnp
from jax import lax
from jax.experimental import pallas as pl
from jax.experimental.pallas import tpu as pltpu
from jax.sharding import PartitionSpec as P

MESH = pl.DeviceIdType.MESH
HEAD = 256
EPSILON = 1e-05
SCALE = HEAD**-0.5
f32 = jnp.float32
bf16 = jnp.bfloat16
SUBS = 8


def nt(left, right):
    return lax.dot_general(left, right, (((1,), (1,)), ((), ())), preferred_element_type=f32)


def nn(left, right):
    return jnp.dot(left, right, preferred_element_type=f32)


def norm(rows):
    centred = rows - jnp.mean(rows, axis=-1, keepdims=True)
    inverse = lax.rsqrt(jnp.mean(centred * centred, axis=-1, keepdims=True) + EPSILON)
    return centred * inverse, inverse


def norm_back(scaled, inverse, gain, upstream):
    weighted = upstream * gain
    spread = jnp.mean(weighted * scaled, axis=-1, keepdims=True)
    return inverse * (weighted - jnp.mean(weighted, axis=-1, keepdims=True) - scaled * spread)


def loop(start, stop, body):
    lax.fori_loop(start, stop, lambda i, carry: (body(i), carry)[1], 0)


def kernel(names, Z, T, *refs):
    (target_h, source_h, cot_h, tgain, sgain, wq_h, wk_h, wv_h, wo_h, tgrad, sgrad, wgrad) = refs[:12]
    s = SimpleNamespace(**dict(zip(names, refs[12:])))
    D = wq_h.shape[0]
    TR = target_h.shape[0]
    SR = T * source_h.shape[0]
    C = T // 2
    HALF = D // 2
    PART = wk_h.shape[0]
    G = HEAD // PART
    z = lax.axis_index("sp")
    t = lax.axis_index("tp")
    c = lax.rem(t, 2)
    p = lax.div(t, 2)
    other = t + 1 - 2 * c
    j = lax.rem(t, G)

    def remote(src, dst, send, recv, **where):
        return pltpu.make_async_remote_copy(
            src_ref=src, dst_ref=dst, send_sem=send, recv_sem=recv, device_id=where, device_id_type=MESH
        )

    def zat(k):
        return lax.rem(z + k + Z, Z)

    def chip(k):
        return lax.rem(p + k, C)

    def same(k):
        return 2 * chip(k) + c

    def mate(k):
        return t - j + lax.rem(j + k, G)

    row0 = pl.multiple_of(p * (TR // C), TR // C)
    loads = [
        pltpu.make_async_copy(a, b, s.in_sem.at[i])
        for i, (a, b) in enumerate(
            (
                (source_h, s.src),
                (target_h, s.tgt),
                (wq_h, s.wq),
                (cot_h, s.cot),
                (wo_h, s.wo),
                (wk_h, s.wkv.at[0:PART, :]),
                (wv_h, s.wkv.at[PART : 2 * PART, :]),
                (target_h.at[pl.ds(row0, TR // C), :], s.t8),
                (cot_h.at[pl.ds(row0, TR // C), :], s.c8),
            )
        )
    ]
    for one in loads:
        one.start()

    barrier = pltpu.get_barrier_semaphore()

    def greet(**where):
        pl.semaphore_signal(barrier, inc=1, device_id=where, device_id_type=MESH)

    loop(1, Z, lambda k: greet(sp=zat(k)))
    loop(1, C, lambda k: greet(tp=same(k)))
    greet(tp=other)
    greet(tp=mate(2) + 1 - 2 * c)

    loads[0].wait()
    scaled, inverse = norm(s.src[...].astype(f32))
    s.src_scaled[...] = scaled
    s.src_inv[...] = jnp.broadcast_to(inverse, s.src_inv.shape)
    s.g[t] = (scaled * sgain[...]).astype(bf16)
    loads[1].wait()

    def norm_target(i):
        rows = pl.ds(pl.multiple_of(i * 32, 32), 32)
        values, _ = norm(s.tgt[rows, :].astype(f32))
        s.tn[rows, :] = (values * tgain[...]).astype(bf16)

    loop(0, TR // 32, norm_target)
    own = pl.ds(pl.multiple_of(z * TR, TR), TR)
    loads[2].wait()
    s.qd[own, 0:HEAD] = nn(s.tn[...], s.wq[...]).astype(bf16)
    loads[3].wait()
    loads[4].wait()
    s.qd[own, HEAD : 2 * HEAD] = nt(s.cot[...], s.wo[...]).astype(bf16)
    pl.semaphore_wait(barrier, (Z - 1) + (C - 1) + 2)

    def source_copy(k):
        return remote(s.g.at[t], s.g.at[t], s.src_send.at[k], s.src_recv.at[t], tp=same(k))

    loop(1, C, lambda k: source_copy(k).start())

    def forward_copy(k):
        row = s.g.at[same(k)]
        return remote(row, row, s.fwd_send.at[k], s.src_recv.at[same(k)], tp=other)

    forward_copy(0).start()
    rows_sub = TR // SUBS

    def ring_copy(block, sub, way, step):
        rows = s.qd.at[pl.ds(pl.multiple_of(block * TR + sub * rows_sub, rows_sub), rows_sub), :]
        return remote(
            rows, rows, s.ring_send.at[way, step, sub], s.ring_recv.at[way, step, sub],
            sp=zat(1 if way == 0 else -1),
        )

    H = Z // 2

    def reach(way, step):
        if step < H:
            return 0, SUBS
        return (0, SUBS // 2) if way == 0 else (SUBS // 2, SUBS)

    for way in (0, 1):
        loop(*reach(way, 1), lambda sub: ring_copy(z, sub, way, 1).start())

    def ring(step, first=-1):
        def arrive(way, sub, on):
            block = zat(-step if way == 0 else step)
            ring_copy(block, sub, way, step).wait_recv()
            if on:
                ring_copy(block, sub, way, step + 1).start()

        def both(lo, hi, on):
            def at(pair):
                for sub in (2 * pair, 2 * pair + 1):
                    arrive(0, sub, on[0])
                    arrive(1, sub, on[1])
                if first >= 0:
                    scores_sent(first + pair)

            loop(lo // 2, hi // 2, at)

        if step < H - 1:
            both(0, SUBS, (True, True))
        elif step == H - 1:
            both(0, SUBS // 2, (True, False))
            both(SUBS // 2, SUBS, (False, True))
        else:

            def last(sub):
                arrive(0, sub, False)
                arrive(1, SUBS // 2 + sub, False)

            loop(first, 2 * H - 1, scores_sent)
            loop(0, SUBS // 2, last)

    loads[5].wait()
    loads[6].wait()

    ring(1)

    def pass_on(k):
        source_copy_from(k).wait_recv()
        forward_copy(k).start()

    def source_copy_from(k):
        row = s.g.at[same(k)]
        return remote(row, row, s.src_send.at[k], s.src_recv.at[same(k)], tp=other)

    loop(1, C // 2, pass_on)
    ring(2)
    loop(C // 2, C, pass_on)

    def from_other(k):
        at = 2 * chip(k) + 1 - c
        remote(s.g.at[at], s.g.at[at], s.src_send.at[k], s.src_recv.at[at], tp=other).wait_recv()

    ring(3)
    loop(0, C, from_other)

    def stack_rows(q):
        both = jnp.concatenate((s.g[2 * q].astype(f32), s.g[2 * q + 1].astype(f32)), axis=0)
        s.rows[pl.ds(pl.multiple_of(q * 16, 16), 16), :] = both.astype(bf16)

    loop(0, C, stack_rows)
    s.kvp[j] = nt(s.rows[...], s.wkv[...]).astype(bf16)

    def join_copy(k):
        return remote(s.kvp.at[j], s.kvp.at[j], s.join_send.at[k], s.join_recv.at[j], tp=mate(k))

    for k in range(1, G):
        join_copy(k).start()
    ring(4)
    def block_of(k):
        return zat(lax.div(k + 1, 2) * (2 * lax.rem(k, 2) - 1))

    def stat_copy(k):
        b = block_of(k)
        return remote(s.stat.at[b], s.got.at[z], s.stat_send.at[k], s.stat_recv.at[z], sp=lax.rem(b + H, Z))

    def scores(k):
        b = block_of(k)
        rows = pl.ds(pl.multiple_of(b * TR, TR), TR)
        scores_t = nt(s.keys[...], s.qd[rows, 0:HEAD]) * SCALE
        products_t = nt(s.values[...], s.qd[rows, HEAD : 2 * HEAD])
        highest = jnp.max(scores_t, axis=0, keepdims=True)
        weights = jnp.exp(scores_t - highest)
        s.e[b] = weights
        s.p[b] = products_t
        s.stat[b, 0:1, :] = highest
        s.stat[b, 1:2, :] = jnp.sum(weights, axis=0, keepdims=True)
        s.stat[b, 2:3, :] = jnp.sum(weights * products_t, axis=0, keepdims=True)
        s.stat[b, 3:4, :] = highest

    def scores_sent(k):
        scores(k)
        stat_copy(k).start()

    ring(5)
    for k in range(1, G):
        at = lax.rem(j + k, G)
        remote(s.kvp.at[at], s.kvp.at[at], s.join_send.at[k], s.join_recv.at[at], tp=other).wait_recv()
    parts = [s.kvp[i].astype(f32) for i in range(G)]
    keys = jnp.concatenate([a[:, :PART] for a in parts], axis=1)
    s.keys[...] = keys.astype(bf16)
    s.keys_t[...] = keys.T.astype(bf16)
    s.values[...] = jnp.concatenate([a[:, PART:] for a in parts], axis=1).astype(bf16)
    ring(6, 0)
    loop(4, 6, scores_sent)
    ring(7, 6)
    loop(10, 12, scores_sent)
    ring(8, 12)
    scores(15)
    far = zat(H)
    s.got[z] = s.stat[far]

    def stat_wait(k):
        at = block_of(k)
        remote(s.stat.at[at], s.got.at[at], s.stat_send.at[k], s.stat_recv.at[at], sp=at).wait_recv()

    loop(1, Z, stat_wait)
    parts = [s.got[i, 0:1, :] for i in range(Z)]
    top = functools.reduce(jnp.maximum, parts)
    factors = [jnp.exp(a - top) for a in parts]
    total = sum(s.got[i, 1:2, :] * factors[i] for i in range(Z))
    weighted = sum(s.got[i, 2:3, :] * factors[i] for i in range(Z))
    s.fin[far, 0:1, :] = top + jnp.log(total)
    s.fin[far, 1:2, :] = weighted / total

    def fin_copy(k):
        return remote(s.fin.at[far], s.fin.at[far], s.fin_send.at[k], s.fin_recv.at[far], sp=block_of(k))

    loop(1, Z, lambda k: fin_copy(Z - k).start())

    def fin_wait(k):
        at = block_of(k)
        remote(s.fin.at[at], s.fin.at[at], s.fin_send.at[k], s.fin_recv.at[at], sp=at).wait_recv()

    def slopes(b):
        cols = pl.ds(pl.multiple_of(b * TR, TR), TR)
        weights = s.e[b] * jnp.exp(s.stat[b, 0:1, :] - s.fin[b, 0:1, :])
        s.att[:, cols] = weights.astype(bf16)
        s.slo[:, cols] = (weights * (s.p[b] - s.fin[b, 1:2, :]) * SCALE).astype(bf16)

    hd = HEAD // 2
    STEP = 2

    def sign(way, k):
        return zat(k if way == 1 else -k)

    def hops(way, sub):
        return H if way == sub else H - 1

    def dq_copy(way, k, sub):
        return remote(
            s.dq_out.at[way, k, sub], s.dq_in.at[way, k, sub],
            s.dq_send.at[way, k, sub], s.dq_recv.at[way, k, sub],
            sp=sign(way, k % STEP or STEP),
        )

    def dq_sum(way, k, sub):
        b = sign(way, k) if k else z
        total = s.dq[sub * hd : (sub + 1) * hd, pl.ds(pl.multiple_of(b * TR, TR), TR)]
        if k % STEP == 0:
            for way_in in (way,) if k else (0, 1):
                for far_k in range(k + 1, min(k + STEP, hops(way_in, sub)) + 1):
                    dq_copy(way_in, far_k, sub).wait_recv()
                    total = total + s.dq_in[way_in, far_k, sub].astype(f32)
        return total

    def dq_stage(k):
        for sub in (0, 1):
            for way in (0, 1):
                if k <= hops(way, sub):
                    s.dq_out[way, k, sub] = dq_sum(way, k, sub).astype(bf16)
                    dq_copy(way, k, sub).start()

    def settle(k):
        fin_wait(k)
        slopes(block_of(k))

    def part(k):
        cols = pl.ds(pl.multiple_of(block_of(k) * TR, TR), TR)
        s.dq[:, cols] = nn(s.keys_t[...], s.slo[:, cols])

    slopes(far)
    part(2 * H - 1)
    dq_stage(8)
    for k in (13, 14):
        settle(k)
        part(k)
    dq_stage(7)
    for k in (11, 12, 9, 10):
        settle(k)
        part(k)
    dq_stage(5)
    loop(0, 4, lambda i: settle(8 - i))
    dq_stage(6)
    loop(0, 5, lambda i: settle(4 - i))
    def share(i):
        return pl.ds(pl.multiple_of(i * PART, PART), PART)

    def dkv_copy(h, k):
        return remote(
            s.dkv_out.at[h, k], s.dkv_in.at[h, k], s.dkv_send.at[h, k], s.dkv_recv.at[h, k], tp=mate(k)
        )

    for h, left in enumerate((s.slo, s.att)):
        s.dkv[h] = nn(left[...], s.qd[:, h * HEAD : (h + 1) * HEAD]).T
        for k in range(1, G):
            s.dkv_out[h, k] = s.dkv[h, share(lax.rem(j + k, G)), :].astype(bf16)
        for k in range(1, G):
            dkv_copy(h, k).start()

    def group_sum(h):
        total = s.dkv[h, share(j), :]
        for k in range(1, G):
            dkv_copy(h, k).wait_recv()
            total = total + s.dkv_in[h, k].astype(f32)
        return total

    s.dq[...] = nn(s.keys_t[...], s.slo[...])
    dq_stage(3)
    dq_stage(4)
    keys_part = group_sum(0)
    part_t = nn(keys_part.astype(bf16), s.rows[...])
    CW = D // Z
    for i in range(Z):
        s.wp[i] = part_t[:, i * CW : (i + 1) * CW].astype(bf16)
    R = H // 2

    def w_copy(way, k):
        hop = k % R or R
        src = s.w_rel.at[way] if k == R else s.wp.at[sign(way, k)]
        return remote(src, s.w_in.at[way, k], s.w_send.at[way, k], s.w_recv.at[way, k], sp=sign(way, hop))

    top_hop = (2 * R, 2 * R - 1)
    for way in (0, 1):
        for k in range(top_hop[way], R, -1):
            w_copy(way, k).start()

    def w_relay():
        for way in (0, 1):
            total = s.wp[sign(way, R)].astype(f32)
            for k in range(R + 1, top_hop[way] + 1):
                w_copy(way, k).wait_recv()
                total = total + s.w_in[way, k].astype(f32)
            s.w_rel[way] = total.astype(bf16)
            w_copy(way, R).start()

    def f_copy(way, k, relay):
        block = sign(1 - way, R) if relay else z
        hop = k - R if relay else k
        return remote(s.wf.at[block], s.wf.at[block], s.f_send.at[way, k], s.f_recv.at[block], sp=sign(way, hop))

    def w_owner():
        total = s.wp[z].astype(f32)
        for way in (0, 1):
            for k in range(1, R + 1):
                w_copy(way, k).wait_recv()
                total = total + s.w_in[way, k].astype(f32)
        s.wf[z] = total.astype(bf16)
        for way in (0, 1):
            for k in range(R, 0, -1):
                f_copy(way, k, False).start()

    def f_wait(k):
        at = block_of(k)
        remote(s.wf.at[at], s.wf.at[at], s.f_send.at[0, k % 2], s.f_recv.at[at], sp=at).wait_recv()

    def f_relay():
        for way in (0, 1):
            f_wait(2 * R - 1 if way == 0 else 2 * R)
            for k in range(top_hop[way], R, -1):
                f_copy(way, k, True).start()

    dq_stage(1)
    s.flat[...] = jnp.concatenate((keys_part, group_sum(1)), axis=0).T.astype(bf16)
    s.su[...] = nn(s.flat[...], s.wkv[...])

    def for_other(q):
        s.ss[q] = s.su[pl.ds(pl.multiple_of(q * 16 + 8 * (1 - c), 8), 8), :].astype(bf16)

    loop(0, C, for_other)
    su_pair = remote(s.ss, s.sr, s.pair_send.at[0], s.pair_recv.at[0], tp=other)
    su_pair.start()
    dq_stage(2)
    for way in (0, 1):
        for k in range(R - 1, 0, -1):
            w_copy(way, k).start()
    su_pair.wait_recv()

    def sw_copy(k):
        return remote(s.sv.at[chip(k)], s.sw.at[p], s.sw_send.at[k], s.sw_recv.at[p], tp=same(k))

    def both_cores(k):
        q = chip(k)
        mine = s.su[pl.ds(pl.multiple_of(q * 16 + 8 * c, 8), 8), :]
        return (mine + s.sr[q].astype(f32)).astype(bf16)

    s.sw[p] = both_cores(0)

    def sw_start(k):
        s.sv[chip(k)] = both_cores(k)
        sw_copy(k).start()

    loop(1, C, sw_start)
    w_relay()
    query_flat = jnp.concatenate([dq_sum(0, 0, sub) for sub in (0, 1)], axis=0).T.astype(bf16)

    TB = TR // C

    def half_cols(h):
        return s.wq[pl.ds(pl.multiple_of(h * HALF, HALF), HALF), :]

    s.tsend[...] = nt(query_flat, half_cols(1 - c)).reshape(C, TB, HALF).astype(bf16)
    tu_pair = remote(s.tsend, s.trecv, s.pair_send.at[1], s.pair_recv.at[1], tp=other)
    tu_pair.start()
    s.tmine[...] = nt(query_flat, half_cols(c)).reshape(C, TB, HALF)

    def sw_wait(k):
        at = chip(k)
        remote(s.sv.at[at], s.sw.at[at], s.sw_send.at[k], s.sw_recv.at[at], tp=other).wait_recv()

    w_owner()
    tu_pair.wait_recv()

    def tw_copy(k):
        return remote(s.tv.at[chip(k)], s.tw.at[p], s.tw_send.at[k], s.tw_recv.at[p], tp=same(k))

    def tboth(k):
        q = chip(k)
        return (s.tmine[q] + s.trecv[q].astype(f32)).astype(bf16)

    s.tw[p] = tboth(0)

    def tw_start(k):
        s.tv[chip(k)] = tboth(k)
        tw_copy(k).start()

    loop(1, C, tw_start)

    loop(1, C, sw_wait)
    s.su8[...] = s.sw[0].astype(f32)

    def add_sw(i):
        s.su8[...] += s.sw[i].astype(f32)

    loop(1, C, add_sw)
    sgrad[...] = norm_back(s.src_scaled[...], s.src_inv[:, 0:1], sgain[...], s.su8[...])
    f_relay()
    loop(1, C, lambda k: source_copy(k).wait_send())
    loop(0, C, lambda k: forward_copy(k).wait_send())
    for way in (0, 1):
        for step in range(1, H + 1):
            block = zat(-(step - 1) if way == 0 else step - 1)
            loop(*reach(way, step), lambda sub: ring_copy(block, sub, way, step).wait_send())
    for k in range(1, G):
        join_copy(k).wait_send()
        dkv_copy(0, k).wait_send()
        dkv_copy(1, k).wait_send()

    def line_sends(k):
        stat_copy(k - 1).wait_send()
        fin_copy(k).wait_send()

    loop(1, Z, line_sends)
    for way in (0, 1):
        for sub in (0, 1):
            for k in range(1, hops(way, sub) + 1):
                dq_copy(way, k, sub).wait_send()
        for k in range(1, top_hop[way] + 1):
            w_copy(way, k).wait_send()
    su_pair.wait_send()
    loop(1, C, lambda k: sw_copy(k).wait_send())

    def tw_wait(k):
        at = chip(k)
        remote(s.tv.at[at], s.tw.at[at], s.tw_send.at[k], s.tw_recv.at[at], tp=other).wait_recv()

    loop(1, C, tw_wait)
    s.tu8[...] = s.tw[0].astype(f32)

    def add_tw(i):
        s.tu8[...] += s.tw[i].astype(f32)

    loop(1, C, add_tw)
    TO = TB // 2
    lower, upper = s.tu8[0:TO, :], s.tu8[TO:TB, :]
    mine = jnp.where(c == 0, lower, upper)
    s.tx_out[...] = jnp.where(c == 0, upper, lower)
    last_pair = remote(s.tx_out, s.tx_in, s.pair_send.at[2], s.pair_recv.at[2], tp=other)
    last_pair.start()
    loads[7].wait()
    loads[8].wait()
    scaled, inverse = norm(s.t8[...].astype(f32))
    cot = s.c8[...].astype(f32)
    scaled = jnp.where(c == 0, scaled[0:TO], scaled[TO:TB])
    inverse = jnp.where(c == 0, inverse[0:TO], inverse[TO:TB])
    cot = jnp.where(c == 0, cot[0:TO], cot[TO:TB])
    last_pair.wait_recv()
    theirs = s.tx_in[...]
    upstream = jnp.concatenate(
        (jnp.where(c == 0, mine, theirs), jnp.where(c == 0, theirs, mine)), axis=1
    )
    tgrad[...] = cot + norm_back(scaled, inverse, tgain[...], upstream)

    for k in range(1, Z):
        if k not in (2 * R - 1, 2 * R):
            f_wait(k)
    for i in range(Z):
        wgrad[:, i * CW : (i + 1) * CW] = s.wf[i]
    for way in (0, 1):
        for k in range(1, top_hop[way] + 1):
            f_copy(way, k, k > R).wait_send()
    loop(1, C, lambda k: tw_copy(k).wait_send())
    tu_pair.wait_send()
    last_pair.wait_send()


def put(tgrad, sgrad, wgrad, tgrad_out, sgrad_out, wgrad_out):
    tgrad_out[...] = tgrad[...]
    sgrad_out[...] = sgrad[...]
    wgrad_out[...] = wgrad[...].astype(f32)


def solution(mesh):
    Z, T = mesh.shape["sp"], mesh.shape["tp"]

    def on_device(target, source, cotangent, target_gain, source_gain, wq, wk, wv, wo):
        TR, D = target.shape
        SB = source.shape[0]
        SR = SB * T
        C = T // 2
        PART = wk.shape[1]
        G = HEAD // PART
        H = Z // 2
        TB = TR // C
        CW = D // Z
        V = pltpu.VMEM
        dma = pltpu.SemaphoreType.DMA
        scratch = dict(
            src=V((SB, D), bf16), tgt=V((TR, D), bf16), cot=V((TR, D), bf16),
            wq=V((D, HEAD), bf16), wo=V((HEAD, D), bf16),
            t8=V((TB, D), bf16), c8=V((TB, D), bf16),
            src_scaled=V((SB, D), f32), src_inv=V((SB, 128), f32),
            g=V((T, SB, D), bf16), tn=V((TR, D), bf16), qd=V((Z * TR, 2 * HEAD), bf16),
            wkv=V((2 * PART, D), bf16), rows=V((SR, D), bf16), kvp=V((G, SR, 2 * PART), bf16),
            keys=V((SR, HEAD), bf16), keys_t=V((HEAD, SR), bf16), values=V((SR, HEAD), bf16),
            e=V((Z, SR, TR), f32), p=V((Z, SR, TR), f32),
            stat=V((Z, 4, TR), f32), got=V((Z, 4, TR), f32), fin=V((Z, 2, TR), f32),
            att=V((SR, Z * TR), bf16), slo=V((SR, Z * TR), bf16), dq=V((HEAD, Z * TR), f32),
            dq_out=V((2, H + 1, 2, HEAD // 2, TR), bf16), dq_in=V((2, H + 1, 2, HEAD // 2, TR), bf16),
            dkv=V((2, HEAD, SR), f32), dkv_out=V((2, G, PART, SR), bf16), dkv_in=V((2, G, PART, SR), bf16),
            flat=V((SR, 2 * PART), bf16),
            wp=V((Z, PART, CW), bf16), w_in=V((2, H + 1, PART, CW), bf16), w_rel=V((2, PART, CW), bf16),
            wf=V((Z, PART, CW), bf16),
            su=V((SR, D), f32), ss=V((C, SB, D), bf16), sr=V((C, SB, D), bf16),
            sv=V((C, SB, D), bf16), sw=V((C, SB, D), bf16), su8=V((SB, D), f32),
            tsend=V((C, TB, D // 2), bf16), trecv=V((C, TB, D // 2), bf16), tmine=V((C, TB, D // 2), f32),
            tv=V((C, TB, D // 2), bf16), tw=V((C, TB, D // 2), bf16), tu8=V((TB, D // 2), f32),
            tx_out=V((TB // 2, D // 2), f32), tx_in=V((TB // 2, D // 2), f32),
            in_sem=dma((9,)), src_send=dma((C,)), fwd_send=dma((C,)), src_recv=dma((T,)),
            ring_send=dma((2, H + 1, SUBS)), ring_recv=dma((2, H + 1, SUBS)),
            join_send=dma((G,)), join_recv=dma((G,)), dkv_send=dma((2, G)), dkv_recv=dma((2, G)),
            stat_send=dma((Z,)), stat_recv=dma((Z,)), fin_send=dma((Z,)), fin_recv=dma((Z,)),
            w_send=dma((2, H + 1)), w_recv=dma((2, H + 1)), f_send=dma((2, H + 1)), f_recv=dma((Z,)),
            dq_send=dma((2, H + 1, 2)), dq_recv=dma((2, H + 1, 2)),
            sw_send=dma((C,)), sw_recv=dma((C,)), tw_send=dma((C,)), tw_recv=dma((C,)),
            pair_send=dma((3,)), pair_recv=dma((3,)),
        )
        vmem = pl.BlockSpec(memory_space=pltpu.VMEM)
        any_ = pl.BlockSpec(memory_space=pl.ANY)
        tgrad, sgrad, wgrad = pl.pallas_call(
            functools.partial(kernel, tuple(scratch), Z, T),
            out_shape=(
                jax.ShapeDtypeStruct((TR // T, D), f32),
                jax.ShapeDtypeStruct((SB, D), f32),
                jax.ShapeDtypeStruct((PART, D), bf16),
            ),
            in_specs=[any_, any_, any_, vmem, vmem, any_, any_, any_, any_],
            out_specs=(vmem, vmem, vmem),
            scratch_shapes=list(scratch.values()),
            compiler_params=pltpu.CompilerParams(
                collective_id=0, has_side_effects=True, vmem_limit_bytes=62 * 1024 * 1024
            ),
            name="backward",
        )(target, source, cotangent, target_gain.reshape(1, D), source_gain.reshape(1, D), wq, wk.T, wv.T, wo)
        tgrad, sgrad, wgrad = pl.pallas_call(
            put,
            out_shape=(
                jax.ShapeDtypeStruct((TR // T, D), f32),
                jax.ShapeDtypeStruct((SB, D), f32),
                jax.ShapeDtypeStruct((PART, D), f32),
            ),
            in_specs=[vmem, vmem, vmem],
            out_specs=(vmem, vmem, vmem),
            name="put",
        )(tgrad, sgrad, wgrad)
        return tgrad, sgrad, wgrad.T

    return jax.shard_map(
        on_device,
        mesh=mesh,
        in_specs=(
            P("sp", None), P(("sp", "tp"), None), P("sp", None), P(), P(),
            P(None, "tp"), P(None, "tp"), P(None, "tp"), P("tp", None),
        ),
        out_specs=(P(("sp", "tp"), None), P(("sp", "tp"), None), P(None, "tp")),
        check_vma=False,
    )
```
